32 devices in a mesh: st: 16 (over z, y, x), tp: 2 (over core).
Axes of the slice: x: 2, y: 2, z: 4, core: 2. Of those that a mesh axis runs over, the one named last changes fastest.
Arguments:
- tokens: bfloat16 [16384, 2048], P('st', 'tp'), may hold values from -6 to 6
- passage_ids: int32 [256, 2], P('st'), may hold values from 0 to 255, as said below
- passage_store: bfloat16 [256, 64, 2048], P('st'), may hold values from -6 to 6
- norm_gain: bfloat16 [2048], replicated, may hold values from 0.099609375 to 1.8984375
- conv_value_weight: bfloat16 [2048, 1536], P(None, 'tp'), may hold values from -0.125 to 0.125
- conv_gate_weight: bfloat16 [2048, 1536], P(None, 'tp'), may hold values from -0.125 to 0.125
- conv_weight: bfloat16 [31, 1536], P(None, 'tp'), may hold values from -1 to 1
- ln_gain: bfloat16 [1536], P('tp'), may hold values from 0.099609375 to 1.8984375
- query_weight: bfloat16 [2048, 512], P(None, 'tp'), may hold values from -0.125 to 0.125
- query_gain: bfloat16 [512], P('tp'), may hold values from 0.5 to 10
- passage_gain: bfloat16 [2048], replicated, may hold values from 0.099609375 to 1.8984375
- key_weight: bfloat16 [2048, 512], P(None, 'tp'), may hold values from -0.125 to 0.125
- value_weight: bfloat16 [2048, 512], P(None, 'tp'), may hold values from -0.125 to 0.125
- key_gain: bfloat16 [512], P('tp'), may hold values from 0.5 to 10
- memory_gate: bfloat16 [512], P('tp'), may hold values from 0.29882812 to 1.5
- conv_out_weight: bfloat16 [1536, 2048], P('tp'), may hold values from -0.125 to 0.125
- memory_out_weight: bfloat16 [512, 2048], P('tp'), may hold values from -0.125 to 0.125
Outputs:
- layer_out: bfloat16 [16384, 2048], P(('st', 'tp'))
The draws below stay inside these ranges and needn't reach their ends.
Inputs may be any that keep to these rules, and one draw needn't show every extreme that they name: The owner of passage p is p // 16. Among the 32 entries of the rows of passage_ids that lie on one index of st (aligned runs of 16 rows, that is the blocks of one index of st), no owner is named more than 4 times, and in every such run some owner is named exactly 4 times.
All inputs are finite; a program needn't handle non-finite values.
Results may differ from the reference program's by a relative error of at most 0.008.
The reference program's roundings to bfloat16 on the way count: a program that leaves them out, or rounds other values in their place, can miss the bound.
Values may be sent and summed in bfloat16 or wider, within the bound.
A program may use at most 192 MiB of HBM per device.

```python
import jax
import jax.numpy as jnp
from jax import lax

D = 2048
C_A = 1536
MEM_HEADS = 8
MEM_HD = 64
MEM_W = 512
KW = 31
TOK_DEV = 1024
SEQS_DEV = 2
SEQ_LEN = 512
BLOCK = 64
PASS = 2
PLEN = 64
PASS_DEV = 16
TOKENS = 16384
BLOCKS = 256
PASSAGES = 256
N_ST = 16
N_TP = 2


def draw_passage_ids(key, part):
    owner_count = PASSAGES // PASS_DEV
    blocks_each = BLOCKS // owner_count
    request_count = blocks_each * PASS
    most_each = max(1, 2 * request_count // owner_count)
    slot_count = owner_count * most_each
    popular_key, hot_key, device_key = jax.random.split(jax.random.fold_in(key, 3), 3)
    popular = jax.random.randint(popular_key, (owner_count,), 0, 256)
    popular = popular * popular
    hot_owner = jax.random.randint(hot_key, (), 0, owner_count)
    slot_range = jnp.arange(slot_count, dtype=jnp.int32)
    slot_owner = slot_range // most_each
    first_slot = slot_range % most_each == 0

    def one_device(device):
        score_key, local_key, other_key, order_key = jax.random.split(jax.random.fold_in(device_key, device), 4)
        before = (device + owner_count - 1) % owner_count
        across = (device + owner_count // 2) % owner_count
        forced = (slot_owner == hot_owner) | first_slot & ((slot_owner == before) | (slot_owner == across))
        scores = jax.random.randint(score_key, (slot_count,), 0, 1 << 16) + popular[slot_owner] + jnp.where(forced, 1 << 18, 0)
        _, chosen = lax.top_k(scores * slot_count + slot_range, request_count)
        local_index = jnp.minimum(jax.random.randint(local_key, (request_count,), 0, PASS_DEV), jax.random.randint(other_key, (request_count,), 0, PASS_DEV))
        order = jax.random.permutation(order_key, request_count)
        picked = chosen // most_each * PASS_DEV + local_index
        return picked[order].reshape(blocks_each, PASS)
    return jax.vmap(one_device)(jnp.arange(owner_count, dtype=jnp.int32)).reshape(BLOCKS, PASS).astype(jnp.int32)


def gain_law(key):
    return jax.random.uniform(key, (MEM_W,), jnp.float32, 0.5, 2.5)


def draw_query_gain(key, part):
    return gain_law(jax.random.fold_in(key, 11)).astype(jnp.bfloat16)


def draw_key_gain(key, part):
    return gain_law(jax.random.fold_in(key, 17)).astype(jnp.bfloat16)


def draw_conv_weight(key, part):
    base = jax.random.truncated_normal(jax.random.fold_in(key, 23), -3.0, 3.0, (KW, C_A), jnp.float32)
    channel_scale = jnp.where(jnp.arange(C_A) < C_A // 2, 2.0, 0.6) * KW ** (-0.5)
    return jnp.clip(base * channel_scale[None, :], -1.0, 1.0).astype(jnp.bfloat16)


def shard_levels(key, shape, shards, low, largest):
    gain, own = 1.0, jax.random.fold_in(key, 6)
    for dim, blocks in shards:
        draws = jnp.exp(jax.random.uniform(jax.random.fold_in(own, dim), (blocks,), jnp.float32, low / len(shards), largest / len(shards)))
        gain = gain * jnp.repeat(draws, shape[dim] // blocks).reshape([-1 if axis == dim else 1 for axis in range(len(shape))])
    return gain


def gaussian(key, shape, spread, reach, shards=(), kind=jnp.bfloat16):
    array = jax.random.normal(key, shape, jnp.float32) * spread
    if len(shards) > 0:
        array = shard_levels(key, shape, shards, -0.22, 0.18) * array
    return jnp.clip(array, min=-reach, max=reach).astype(kind)


def setup_inputs(seed: int = 0) -> dict:
    streams_of = jax.random.split(jax.random.key(seed), 18)
    tokens = gaussian(streams_of[0], (TOKENS, D), 1.0, 6.0, ((0, 16), (1, 2)))
    passage_ids = draw_passage_ids(jax.random.fold_in(streams_of[17], 71), 0)
    passage_store = gaussian(streams_of[2], (PASSAGES, PLEN, D), 1.0, 6.0, ((0, 16),))
    norm_gain = jnp.clip(1.0 + 0.18 * jax.random.normal(streams_of[3], (D,), jnp.float32), 0.099609375, 1.8984375).astype(jnp.bfloat16)
    conv_value_weight = gaussian(streams_of[4], (D, C_A), D ** -0.5, 0.125, ((1, 2),))
    conv_gate_weight = gaussian(streams_of[5], (D, C_A), D ** -0.5, 0.125, ((1, 2),))
    conv_weight = draw_conv_weight(jax.random.fold_in(streams_of[17], 71), 0)
    ln_gain = jnp.clip(1.0 + 0.18 * jax.random.normal(streams_of[7], (C_A,), jnp.float32), 0.099609375, 1.8984375).astype(jnp.bfloat16)
    query_weight = gaussian(streams_of[8], (D, MEM_W), D ** -0.5, 0.125, ((1, 2),))
    query_gain = draw_query_gain(jax.random.fold_in(streams_of[17], 71), 0)
    passage_gain = jnp.clip(1.0 + 0.18 * jax.random.normal(streams_of[10], (D,), jnp.float32), 0.099609375, 1.8984375).astype(jnp.bfloat16)
    key_weight = gaussian(streams_of[11], (D, MEM_W), D ** -0.5, 0.125, ((1, 2),))
    value_weight = gaussian(streams_of[12], (D, MEM_W), D ** -0.5, 0.125, ((1, 2),))
    key_gain = draw_key_gain(jax.random.fold_in(streams_of[17], 71), 0)
    memory_gate = jnp.clip(0.29882812 + 1.2011719 * jax.random.uniform(streams_of[14], (MEM_W,), jnp.float32) ** shard_levels(streams_of[14], (MEM_W,), ((0, 2),), -0.2, 0.2), 0.29882812, 1.5).astype(jnp.bfloat16)
    conv_out_weight = gaussian(streams_of[15], (C_A, D), (C_A + MEM_W) ** -0.5, 0.125, ((0, 2),))
    memory_out_weight = gaussian(streams_of[16], (MEM_W, D), (C_A + MEM_W) ** -0.5, 0.125, ((0, 2),))
    return {"tokens": tokens, "passage_ids": passage_ids, "passage_store": passage_store, "norm_gain": norm_gain, "conv_value_weight": conv_value_weight, "conv_gate_weight": conv_gate_weight, "conv_weight": conv_weight, "ln_gain": ln_gain, "query_weight": query_weight, "query_gain": query_gain, "passage_gain": passage_gain, "key_weight": key_weight, "value_weight": value_weight, "key_gain": key_gain, "memory_gate": memory_gate, "conv_out_weight": conv_out_weight, "memory_out_weight": memory_out_weight}


NORM_EPS = 1e-06
LAYER_EPS = 1e-05

def row_norm(matrix, gain_row):
    widened = matrix.astype(jnp.float32)
    factor = lax.rsqrt(lax.optimization_barrier(jnp.mean(widened * widened, axis=-1, keepdims=True)) + NORM_EPS)
    return (widened * factor * gain_row.astype(jnp.float32)).astype(jnp.bfloat16)

def head_norm(product, gain_row, head_count):
    row_count = product.shape[0]
    split_heads = product.reshape(row_count, head_count, -1)
    factor = lax.rsqrt(lax.optimization_barrier(jnp.mean(split_heads * split_heads, axis=-1, keepdims=True)) + NORM_EPS)
    head_gains = gain_row.astype(jnp.float32).reshape(head_count, -1)
    return (split_heads * factor * head_gains).reshape(row_count, -1).astype(jnp.bfloat16)

def reference(tokens, passage_ids, passage_store, norm_gain, conv_value_weight, conv_gate_weight, conv_weight, ln_gain, query_weight, query_gain, passage_gain, key_weight, value_weight, key_gain, memory_gate, conv_out_weight, memory_out_weight):
    block_count = TOK_DEV // BLOCK
    token_groups = tokens.reshape(N_ST, TOK_DEV, D)
    id_groups = passage_ids.reshape(N_ST, block_count * PASS)
    taps = conv_weight.astype(jnp.float32)
    conv_part = C_A // N_TP
    head_part = MEM_W // N_TP

    def one_group(inputs):
        token_block, id_block = inputs
        normed_tokens = row_norm(token_block, norm_gain)
        up_value = jnp.dot(normed_tokens, conv_value_weight, preferred_element_type=jnp.float32)
        up_gate = jnp.dot(normed_tokens, conv_gate_weight, preferred_element_type=jnp.float32)
        gated_rows = (up_value * jax.nn.sigmoid(up_gate)).astype(jnp.bfloat16)
        sequences = gated_rows.astype(jnp.float32).reshape(SEQS_DEV, SEQ_LEN, C_A)
        padded = jnp.pad(sequences, ((0, 0), (KW - 1, 0), (0, 0)))
        filtered = jnp.zeros((SEQS_DEV, SEQ_LEN, C_A), jnp.float32)
        for tap in range(KW):
            filtered = filtered + taps[tap][None, None, :] * padded[:, tap:tap + SEQ_LEN, :]
        filtered = filtered.reshape(TOK_DEV, C_A)
        channel_mean = lax.optimization_barrier(jnp.sum(filtered, axis=-1, keepdims=True)) / C_A
        channel_var = lax.optimization_barrier(jnp.sum(filtered * filtered, axis=-1, keepdims=True)) / C_A - channel_mean * channel_mean
        scaled = (filtered - channel_mean) * lax.rsqrt(channel_var + LAYER_EPS) * ln_gain.astype(jnp.float32)
        conv_out = jax.nn.silu(scaled).astype(jnp.bfloat16)
        queries = head_norm(jnp.dot(normed_tokens, query_weight, preferred_element_type=jnp.float32), query_gain, MEM_HEADS)
        query_block = queries.reshape(block_count, BLOCK, MEM_HEADS, MEM_HD)
        fetched = passage_store[id_block].reshape(-1, D)
        normed_rows = row_norm(fetched, passage_gain)
        key_rows = head_norm(jnp.dot(normed_rows, key_weight, preferred_element_type=jnp.float32), key_gain, MEM_HEADS)
        value_rows = jnp.dot(normed_rows, value_weight, preferred_element_type=jnp.float32).astype(jnp.bfloat16)
        key_rows = key_rows.reshape(block_count, PASS * PLEN, MEM_HEADS, MEM_HD)
        value_rows = value_rows.reshape(block_count, PASS * PLEN, MEM_HEADS, MEM_HD)
        scores = jnp.einsum('nbhd,nkhd->nhbk', query_block.astype(jnp.float32), key_rows.astype(jnp.float32)) * MEM_HD ** (-0.5)
        row_max = lax.optimization_barrier(jnp.max(scores, axis=-1, keepdims=True))
        expanded = jnp.exp(scores - row_max)
        weights = (expanded / lax.optimization_barrier(jnp.sum(expanded, axis=-1, keepdims=True))).astype(jnp.bfloat16)
        attended = jnp.einsum('nhbk,nkhd->nbhd', weights.astype(jnp.float32), value_rows.astype(jnp.float32)).reshape(TOK_DEV, MEM_W)
        memory = (attended * jnp.tanh(memory_gate.astype(jnp.float32))).astype(jnp.bfloat16)
        running_sum = jnp.zeros((TOK_DEV, D), jnp.float32)
        for group_index in range(N_TP):
            conv_lo = group_index * conv_part
            head_lo = group_index * head_part
            partial_value = jnp.dot(conv_out[:, conv_lo:conv_lo + conv_part], conv_out_weight[conv_lo:conv_lo + conv_part], preferred_element_type=jnp.float32)
            partial_value = partial_value + jnp.dot(memory[:, head_lo:head_lo + head_part], memory_out_weight[head_lo:head_lo + head_part], preferred_element_type=jnp.float32)
            rounded = lax.optimization_barrier(partial_value.astype(jnp.bfloat16))
            running_sum = running_sum + rounded.astype(jnp.float32)
        return running_sum.astype(jnp.bfloat16)
    return lax.map(one_group, (token_groups, id_groups)).reshape(-1, D)
```

```python
import functools

import jax
import jax.numpy as jnp
from jax import lax
from jax.experimental import pallas as pl
from jax.experimental.pallas import tpu as pltpu
from jax.sharding import PartitionSpec as P

C_A = 1536
MEM_HD = 64
SEQS_DEV = 2
NORM_EPS = 1e-06
LAYER_EPS = 1e-05
REACH = 2
MESH = pl.DeviceIdType.MESH
OFFSETS = tuple(range(-REACH, REACH + 1))


def head_norm(product, gain_row):
    lane = lax.broadcasted_iota(jnp.int32, product.shape, 1)
    squares = product * product
    scale = jnp.zeros_like(product)
    for head in range(product.shape[1] // MEM_HD):
        inside = (lane >= head * MEM_HD) & (lane < (head + 1) * MEM_HD)
        total = jnp.sum(jnp.where(inside, squares, 0.0), axis=-1, keepdims=True)
        scale = jnp.where(inside, lax.rsqrt(total * (1.0 / MEM_HD) + NORM_EPS), scale)
    return (product * scale * gain_row.astype(jnp.float32)).astype(jnp.bfloat16)


def dot32(left, right):
    return jnp.dot(left, right, preferred_element_type=jnp.float32)


def row_norm(rows, gain_row):
    wide = rows.astype(jnp.float32)
    factor = lax.rsqrt(jnp.mean(wide * wide, axis=-1, keepdims=True) + NORM_EPS)
    return (wide * factor * gain_row.astype(jnp.float32)).astype(jnp.bfloat16)


def split_axis(count):
    plane = 1
    for size in range(1, count + 1):
        if count % size == 0 and size * size <= count:
            plane = size
    return count // plane, plane


def layer_kernel(
    depth,
    plane,
    most,
    passes,
    slots_ref,
    wanted_smem,
    wanted_ref,
    norm_gain_ref,
    passage_gain_ref,
    key_gain_ref,
    query_gain_ref,
    ln_gain_ref,
    gate_ref,
    taps_ref,
    tokens_hbm,
    store_hbm,
    key_w_hbm,
    value_w_hbm,
    query_w_hbm,
    conv_value_hbm,
    conv_gate_hbm,
    conv_out_hbm,
    mem_out_hbm,
    out_hbm,
    key_w,
    value_w,
    query_w,
    conv_value,
    conv_gate,
    conv_out_w,
    mem_out_w,
    store_buf,
    x_buf,
    padded,
    filtered,
    acc,
    queries,
    memory,
    stats,
    stats_in,
    part_out,
    part_in,
    result,
    ids_in,
    ids_smem,
    slots,
    *rest,
):
    columns, rest = dict(zip(OFFSETS, rest[: len(OFFSETS)])), rest[len(OFFSETS) :]
    (
        picked,
        far_picked,
        load_sem,
        store_sem,
        x_sem,
        ids_copy_sem,
        ids_send,
        ids_recv,
        hop_send,
        hop_recv,
        plane_send,
        plane_recv,
        far_send,
        far_recv,
        tp_send,
        tp_recv,
        out_sem,
    ) = rest
    me = lax.axis_index("st")
    tp = lax.axis_index("tp")
    z, p = me // plane, me % plane
    power = plane & (plane - 1) == 0
    passage_len = slots.shape[3]
    store_size = columns[0].shape[0]
    tile_passages = store_buf.shape[1] // passage_len
    tiles = store_size // tile_passages
    tile_rows = tile_passages * passage_len
    tokens, features = x_buf.shape
    half = features // 2
    width = key_w.shape[1]

    def reader_place(step):
        return p ^ step if power else (p + step) % plane

    def asker_place(step):
        return p ^ step if power else (p - step + plane) % plane

    far_planes = [o for o in range(depth) if max(o, depth - 1 - o) > REACH]

    def is_far(other):
        return jnp.abs(other - z) > REACH

    def store_copy(tile):
        return pltpu.make_async_copy(
            store_hbm.at[pl.ds(tile * tile_rows, tile_rows)],
            store_buf.at[tile],
            store_sem.at[tile],
        )

    loads = [
        pltpu.make_async_copy(src, dst, load_sem.at[number])
        for number, (src, dst) in enumerate(
            [
                (key_w_hbm, key_w),
                (value_w_hbm, value_w),
                (query_w_hbm, query_w),
                (conv_value_hbm, conv_value),
                (conv_gate_hbm, conv_gate),
                (conv_out_hbm, conv_out_w),
                (mem_out_hbm, mem_out_w),
            ]
        )
    ]
    mine = pl.ds(pl.multiple_of(tp * half, half), half)
    x_copy = pltpu.make_async_copy(tokens_hbm, x_buf.at[:, mine], x_sem)
    store_copy(0).start()
    loads[0].start()
    loads[1].start()
    for tile in range(1, tiles):
        store_copy(tile).start()
    x_copy.start()
    for load in loads[2:]:
        load.start()

    barrier = pltpu.get_barrier_semaphore()

    def greet(st, core):
        pl.semaphore_signal(barrier, inc=1, device_id=(st, core), device_id_type=MESH)

    greet(me, 1 - tp)
    for step in range(1, plane):
        greet(z * plane + reader_place(step), tp)

    @pl.when(z > 0)
    def _():
        greet(me - plane, tp)

    @pl.when(z < depth - 1)
    def _():
        greet(me + plane, tp)

    met = 1 + plane - 1 + jnp.where(z > 0, 1, 0) + jnp.where(z < depth - 1, 1, 0)
    for other in far_planes:

        @pl.when(is_far(other))
        def _(other=other):
            for place in range(plane):
                greet(other * plane + place, tp)

        met = met + jnp.where(is_far(other), plane, 0)
    pl.semaphore_wait(barrier, met)

    def ids_copy(st, send_slot):
        return pltpu.make_async_remote_copy(
            src_ref=wanted_ref,
            dst_ref=ids_in.at[me],
            send_sem=ids_send.at[send_slot],
            recv_sem=ids_recv.at[me],
            device_id=(st, tp),
            device_id_type=MESH,
        )

    def ids_arrival(st):
        return pltpu.make_async_remote_copy(
            src_ref=wanted_ref,
            dst_ref=ids_in.at[st],
            send_sem=ids_send.at[st],
            recv_sem=ids_recv.at[st],
            device_id=(st, tp),
            device_id_type=MESH,
        )

    def ids_local(st):
        return pltpu.make_async_copy(ids_in.at[st], ids_smem.at[st], ids_copy_sem.at[st])

    def for_askers(action):
        for step in range(1, plane):
            action(z * plane + reader_place(step))
        for other in far_planes:

            @pl.when(is_far(other))
            def _(other=other):
                for place in range(plane):
                    action(other * plane + place)

    for_askers(lambda st: ids_copy(st, st).start())

    swap = pltpu.make_async_remote_copy(
        src_ref=tokens_hbm,
        dst_ref=x_buf.at[:, mine],
        send_sem=tp_send.at[0],
        recv_sem=tp_recv.at[0],
        device_id=(me, 1 - tp),
        device_id_type=MESH,
    )
    swap.start()

    def hop(level, up, tile):
        source = columns[-level if up else level]
        target = columns[-level - 1 if up else level + 1]
        rows = pl.ds(tile * tile_passages, tile_passages)
        return pltpu.make_async_remote_copy(
            src_ref=source.at[rows],
            dst_ref=target.at[rows],
            send_sem=hop_send.at[level, int(up), tile],
            recv_sem=hop_recv.at[level, int(up), tile],
            device_id=(me + plane if up else me - plane, tp),
            device_id_type=MESH,
        )

    def sends(level, up):
        if up:
            return (z >= level) & (z < depth - 1)
        return (z <= depth - 1 - level) & (z > 0)

    def gets(level, up):
        if up:
            return z >= level + 1
        return z <= depth - 2 - level

    def start_hop(level, tile):
        for up in (True, False):

            @pl.when(sends(level, up))
            def _(up=up):
                hop(level, up, tile).start()

    def await_hop(level, tile):
        for up in (True, False):

            @pl.when(gets(level, up))
            def _(up=up):
                hop(level, up, tile).wait_recv()

    def end_hop(level, tile):
        for up in (True, False):

            @pl.when(sends(level, up))
            def _(up=up):
                hop(level, up, tile).wait_send()

    loads[0].wait()
    loads[1].wait()

    @pl.loop(0, tiles)
    def _(tile):
        store_copy(tile).wait()
        normed = row_norm(store_buf[tile], passage_gain_ref[...])
        keys = head_norm(dot32(normed, key_w[...]), key_gain_ref[...])
        values = dot32(normed, value_w[...]).astype(jnp.bfloat16)
        rows = pl.ds(tile * tile_passages, tile_passages)
        columns[0][rows, :, :width] = keys.reshape(tile_passages, passage_len, width)
        columns[0][rows, :, width:] = values.reshape(tile_passages, passage_len, width)
        start_hop(0, tile)

    def take_ids(st):
        ids_arrival(st).wait_recv()
        ids_local(st).start()

    for_askers(take_ids)
    for_askers(lambda st: ids_local(st).wait())

    def plane_copy(offset, step):
        return pltpu.make_async_remote_copy(
            src_ref=picked.at[offset + REACH, step - 1],
            dst_ref=slots.at[z + offset, step],
            send_sem=plane_send.at[offset + REACH, step],
            recv_sem=plane_recv.at[offset + REACH, step],
            device_id=(z * plane + reader_place(step), tp),
            device_id_type=MESH,
        )

    def held(offset):
        return (z + offset >= 0) & (z + offset < depth)

    def deliver(offset):
        @pl.when(held(offset))
        def _():
            owner = (z + offset) * plane + p
            for step in range(plane - 1, -1, -1):
                reader = z * plane + reader_place(step)
                for rank in range(most):
                    entry = owner * most + rank
                    if step == 0:
                        index = wanted_smem[entry]
                        slots[z + offset, 0, rank] = columns[offset][index]
                    else:
                        index = ids_smem[reader, 0, entry]
                        picked[offset + REACH, step - 1, rank] = columns[offset][index]
            for step in range(plane - 1, 0, -1):
                plane_copy(offset, step).start()

    def far_row(other):
        near = jnp.minimum(z, REACH) + REACH + 1
        return jnp.where(other < z, other, jnp.maximum(other - near, 0))

    def far_copy(other, place):
        step = p ^ place if power else (place - p + plane) % plane
        return pltpu.make_async_remote_copy(
            src_ref=far_picked.at[far_row(other), place],
            dst_ref=slots.at[z, step],
            send_sem=far_send.at[other, place],
            recv_sem=far_recv.at[z, step],
            device_id=(other * plane + place, tp),
            device_id_type=MESH,
        )

    def far_arrival(other, step):
        return pltpu.make_async_remote_copy(
            src_ref=far_picked.at[far_row(other), step],
            dst_ref=slots.at[other, step],
            send_sem=far_send.at[other, step],
            recv_sem=far_recv.at[other, step],
            device_id=(other * plane + asker_place(step), tp),
            device_id_type=MESH,
        )

    def deliver_far():
        for other in far_planes:

            @pl.when(is_far(other))
            def _(other=other):
                for place in range(plane):
                    for rank in range(most):
                        index = ids_smem[other * plane + place, 0, me * most + rank]
                        far_picked[far_row(other), place, rank] = columns[0][index]
                for place in range(plane):
                    far_copy(other, place).start()

    deliver(0)

    for load in loads[2:5]:
        load.wait()
    x_copy.wait()
    swap.wait()
    taps = taps_ref.shape[0]
    lead = -(-(taps - 1) // 8) * 8
    length = tokens // SEQS_DEV
    channels = padded.shape[2]
    token_tile = min(256, length)
    per_sequence = length // token_tile
    for sequence in range(SEQS_DEV):
        padded[sequence, :lead, :] = jnp.zeros((lead, channels), jnp.float32)
        padded[sequence, lead + length :, :] = jnp.zeros((8, channels), jnp.float32)

    def project(tile):
        rows = pl.ds(pl.multiple_of(tile * token_tile, token_tile), token_tile)
        normed = row_norm(x_buf[rows, :], norm_gain_ref[...])
        queries[rows, :] = head_norm(dot32(normed, query_w[...]), query_gain_ref[...])
        value = dot32(normed, conv_value[...])
        gate = dot32(normed, conv_gate[...])
        gated = (value * jax.nn.sigmoid(gate)).astype(jnp.bfloat16).astype(jnp.float32)
        sequence, part = tile // per_sequence, tile % per_sequence
        start = pl.multiple_of(lead + part * token_tile, 8)
        padded[sequence, pl.ds(start, token_tile), :] = gated

    token_tiles = tokens // token_tile

    @pl.loop(0, token_tiles)
    def _(tile):
        project(tile)

        @pl.when(tile < tiles - 1)
        def _():
            await_hop(0, tile)
            start_hop(1, tile)

    chunk = 64
    span = chunk + lead + 8
    block_width = 256 if channels % 256 == 0 else channels

    def convolve(sequence):
        @pl.loop(0, length // chunk)
        def _(index):
            base = pl.multiple_of(index * chunk, chunk)
            for left in range(0, channels, block_width):
                cols = slice(left, left + block_width)
                window = padded[sequence, pl.ds(base, span), cols]
                total = jnp.zeros((chunk, block_width), jnp.float32)
                for shift in range(8):
                    moved = window if shift == 0 else pltpu.roll(window, span - shift, 0)
                    for start in range(0, lead + 1, 8):
                        tap = start + shift - (lead - taps + 1)
                        if 0 <= tap < taps:
                            weight = taps_ref[tap : tap + 1, cols].astype(jnp.float32)
                            total += weight * moved[start : start + chunk, :]
                out_rows = pl.ds(pl.multiple_of(sequence * length + base, chunk), chunk)
                filtered[out_rows, cols] = total

    convolve(0)
    for tile in range(min(token_tiles, tiles - 1), tiles):
        await_hop(0, tile)
        start_hop(1, tile)
    for distance in range(1, 2):
        deliver(-distance)
        deliver(distance)
    deliver_far()
    for sequence in range(1, SEQS_DEV):
        convolve(sequence)

    row_tile = 128

    @pl.loop(0, tokens // row_tile)
    def _(tile):
        rows = pl.ds(pl.multiple_of(tile * row_tile, row_tile), row_tile)
        block = filtered[rows, :]
        lane = lax.broadcasted_iota(jnp.int32, (row_tile, 128), 1)
        first = jnp.sum(block, axis=-1, keepdims=True)
        second = jnp.sum(block * block, axis=-1, keepdims=True)
        stats[rows, :] = jnp.where(lane == 0, first, second)

    def tp_copy(number, source, target):
        return pltpu.make_async_remote_copy(
            src_ref=source,
            dst_ref=target,
            send_sem=tp_send.at[number],
            recv_sem=tp_recv.at[number],
            device_id=(me, 1 - tp),
            device_id_type=MESH,
        )

    stats_copy = tp_copy(1, stats, stats_in)
    stats_copy.start()
    loads[5].wait()
    loads[6].wait()
    stats_copy.wait()

    @pl.loop(0, tokens // row_tile)
    def _(tile):
        rows = pl.ds(pl.multiple_of(tile * row_tile, row_tile), row_tile)
        sums = stats[rows, :] + stats_in[rows, :]
        mean = sums[:, 0:1] / C_A
        variance = sums[:, 1:2] / C_A - mean * mean
        scaled = (
            (filtered[rows, :] - mean)
            * lax.rsqrt(variance + LAYER_EPS)
            * ln_gain_ref[...].astype(jnp.float32)
        )
        acc[rows, :] = dot32(jax.nn.silu(scaled).astype(jnp.bfloat16), conv_out_w[...])

    for tile in range(tiles):
        await_hop(1, tile)
    for distance in range(2, REACH + 1):
        deliver(-distance)
        deliver(distance)
    for offset in OFFSETS:

        @pl.when(held(offset))
        def _(offset=offset):
            for step in range(1, plane):
                plane_copy(offset, step).wait_recv()

    for other in far_planes:

        @pl.when(is_far(other))
        def _(other=other):
            for step in range(plane):
                far_arrival(other, step).wait_recv()

    heads = width // MEM_HD
    blocks = slots_ref.shape[0] // passes
    block = tokens // blocks
    head_of = lax.broadcasted_iota(jnp.int32, (heads * block, width), 1) // MEM_HD
    row_head = lax.broadcasted_iota(jnp.int32, (heads * block, width), 0) // block
    inside = head_of == row_head
    gate = jnp.tanh(gate_ref[...].astype(jnp.float32))

    def attend(first, count):
        @pl.loop(0, count, unroll=4 if count % 4 == 0 else 1)
        def _(number):
            index = first + number
            rows = pl.ds(pl.multiple_of(index * block, block), block)
            query = queries[rows, :]
            stacked = jnp.concatenate([query] * heads, axis=0)
            stacked = jnp.where(inside, stacked, jnp.zeros_like(stacked))
            read = []
            for part in range(passes):
                slot = slots_ref[index * passes + part]
                read.append(slots[slot // (plane * most), slot // most % plane, slot % most])
            keys = jnp.concatenate([part[:, :width] for part in read], axis=0)
            values = jnp.concatenate([part[:, width:] for part in read], axis=0)
            scores = lax.dot_general(
                stacked, keys, (((1,), (1,)), ((), ())), preferred_element_type=jnp.float32
            ) * MEM_HD ** (-0.5)
            expanded = jnp.exp(scores - jnp.max(scores, axis=-1, keepdims=True))
            weights = (expanded / jnp.sum(expanded, axis=-1, keepdims=True)).astype(jnp.bfloat16)
            mixed = jnp.where(inside, dot32(weights, values), 0.0)
            attended = mixed[:block]
            for head in range(1, heads):
                attended = attended + mixed[head * block : (head + 1) * block]
            memory[rows, :] = (attended * gate).astype(jnp.bfloat16)

    share = tokens // 2
    pieces = part_out.shape[0]
    piece = share // pieces
    theirs, ours = (1 - tp) * share, tp * share
    attend((1 - tp) * (blocks // 2), blocks // 2)
    part_copies = [tp_copy(2 + n, part_out.at[n], part_in.at[n]) for n in range(pieces)]
    for number in range(pieces):
        rows = pl.ds(pl.multiple_of(theirs + number * piece, piece), piece)
        part_out[number] = (acc[rows, :] + dot32(memory[rows, :], mem_out_w[...])).astype(
            jnp.bfloat16
        )
        part_copies[number].start()
    attend(tp * (blocks // 2), blocks // 2)
    out_copies = [
        pltpu.make_async_copy(
            result.at[n], out_hbm.at[pl.ds(n * piece, piece)], out_sem.at[n]
        )
        for n in range(pieces)
    ]
    for number in range(pieces):
        rows = pl.ds(pl.multiple_of(ours + number * piece, piece), piece)
        kept = (acc[rows, :] + dot32(memory[rows, :], mem_out_w[...])).astype(jnp.bfloat16)
        part_copies[number].wait()
        result[number] = (
            kept.astype(jnp.float32) + part_in[number].astype(jnp.float32)
        ).astype(jnp.bfloat16)
        out_copies[number].start()

    for_askers(lambda st: ids_copy(st, st).wait_send())
    for level in range(REACH):
        for tile in range(tiles):
            end_hop(level, tile)
    for offset in OFFSETS:

        @pl.when(held(offset))
        def _(offset=offset):
            for step in range(1, plane):
                plane_copy(offset, step).wait_send()

    for other in far_planes:

        @pl.when(is_far(other))
        def _(other=other):
            for place in range(plane):
                far_copy(other, place).wait_send()

    for copy in out_copies:
        copy.wait()


def layer(
    tokens,
    passage_ids,
    passage_store,
    norm_gain,
    conv_value_weight,
    conv_gate_weight,
    conv_weight,
    ln_gain,
    query_weight,
    query_gain,
    passage_gain,
    key_weight,
    value_weight,
    key_gain,
    memory_gate,
    conv_out_weight,
    memory_out_weight,
):
    owner_count = lax.axis_size("st")
    me = lax.axis_index("st").astype(jnp.int32)
    depth, plane = split_axis(owner_count)
    power = plane & (plane - 1) == 0
    store_size, passage_len, features = passage_store.shape
    count, _ = tokens.shape
    width = key_weight.shape[1]
    channels = conv_weight.shape[1]

    flat_ids = passage_ids.reshape(-1)
    request_count = flat_ids.shape[0]
    most = max(1, 2 * request_count // owner_count)
    owner_index = flat_ids // store_size
    local_index = flat_ids % store_size
    same = (owner_index[:, None] == owner_index[None, :]) & (
        jnp.arange(request_count)[:, None] > jnp.arange(request_count)[None, :]
    )
    rank = jnp.sum(same.astype(jnp.int32), axis=1)
    place, my_place = owner_index % plane, me % plane
    step_to = (place ^ my_place) if power else (my_place - place + plane) % plane
    slot_index = ((owner_index // plane) * plane + step_to) * most + rank
    entry = owner_index * most + rank
    wide = -(-owner_count * most // 128) * 128
    onehot = (entry[:, None] == jnp.arange(wide, dtype=jnp.int32)[None, :]).astype(jnp.int32)
    wanted = jnp.sum(onehot * local_index[:, None], axis=0)

    tile_passages = max(1, min(256 // passage_len, store_size))
    tiles = store_size // tile_passages
    lead = -(-(conv_weight.shape[0] - 1) // 8) * 8
    length = count // SEQS_DEV
    share = count // 2
    pieces = 2
    row = (passage_len, 2 * width)
    bf16, f32 = jnp.bfloat16, jnp.float32
    vmem = pl.BlockSpec(memory_space=pltpu.VMEM)
    smem = pl.BlockSpec(memory_space=pltpu.SMEM)
    anywhere = pl.BlockSpec(memory_space=pl.ANY)
    dma = pltpu.SemaphoreType.DMA
    weights = (
        key_weight,
        value_weight,
        query_weight,
        conv_value_weight,
        conv_gate_weight,
        conv_out_weight,
        memory_out_weight,
    )
    reach = len(OFFSETS)
    scratch = (
        [pltpu.VMEM(w.shape, bf16) for w in weights]
        + [
            pltpu.VMEM((tiles, tile_passages * passage_len, features), bf16),
            pltpu.VMEM((count, features), bf16),
            pltpu.VMEM((SEQS_DEV, lead + length + 8, channels), f32),
            pltpu.VMEM((count, channels), f32),
            pltpu.VMEM((count, features), f32),
            pltpu.VMEM((count, width), bf16),
            pltpu.VMEM((count, width), bf16),
            pltpu.VMEM((count, 128), f32),
            pltpu.VMEM((count, 128), f32),
            pltpu.VMEM((pieces, share // pieces, features), bf16),
            pltpu.VMEM((pieces, share // pieces, features), bf16),
            pltpu.VMEM((pieces, share // pieces, features), bf16),
            pltpu.VMEM((owner_count, 1, wide), jnp.int32),
            pltpu.SMEM((owner_count, 1, wide), jnp.int32),
            pltpu.VMEM((depth, plane, most) + row, bf16),
        ]
        + [pltpu.VMEM((store_size,) + row, bf16) for _ in OFFSETS]
        + [
            pltpu.VMEM((reach, max(plane - 1, 1), most) + row, bf16),
            pltpu.VMEM((max(depth - 1 - REACH, 1), plane, most) + row, bf16),
            dma((len(weights),)),
            dma((tiles,)),
            dma,
            dma((owner_count,)),
            dma((owner_count,)),
            dma((owner_count,)),
            dma((REACH, 2, tiles)),
            dma((REACH, 2, tiles)),
            dma((reach, plane)),
            dma((reach, plane)),
            dma((depth, plane)),
            dma((depth, plane)),
            dma((2 + pieces,)),
            dma((2 + pieces,)),
            dma((pieces,)),
        ]
    )
    return pl.pallas_call(
        functools.partial(layer_kernel, depth, plane, most, passage_ids.shape[1]),
        in_specs=[smem, smem] + [vmem] * 8 + [anywhere] * (2 + len(weights)),
        out_specs=anywhere,
        out_shape=jax.ShapeDtypeStruct((share, features), bf16),
        scratch_shapes=scratch,
        compiler_params=pltpu.CompilerParams(
            collective_id=0, has_side_effects=True, vmem_limit_bytes=67043328
        ),
        cost_estimate=pl.CostEstimate(
            flops=16 << 30, bytes_accessed=24 << 20, transcendentals=0
        ),
        name="layer",
    )(
        slot_index,
        wanted,
        wanted[None, :],
        norm_gain[None, :],
        passage_gain[None, :],
        key_gain[None, :],
        query_gain[None, :],
        ln_gain[None, :],
        memory_gate[None, :],
        conv_weight,
        tokens,
        passage_store.reshape(-1, features),
        *weights,
    )


def solution(mesh):
    return jax.shard_map(
        layer,
        mesh=mesh,
        in_specs=(
            P("st", "tp"),
            P("st", None),
            P("st", None, None),
            P(),
            P(None, "tp"),
            P(None, "tp"),
            P(None, "tp"),
            P("tp"),
            P(None, "tp"),
            P("tp"),
            P(),
            P(None, "tp"),
            P(None, "tp"),
            P("tp"),
            P("tp"),
            P("tp", None),
            P("tp", None),
        ),
        out_specs=P(("st", "tp"), None),
        check_vma=False,
    )
```

```python
import functools

import jax
import jax.numpy as jnp
from jax import lax
from jax.experimental import pallas as pl
from jax.experimental.pallas import tpu as pltpu
from jax.sharding import PartitionSpec as P

C_A = 1536
MEM_HD = 64
SEQS_DEV = 2
NORM_EPS = 1e-06
LAYER_EPS = 1e-05
REACH = 2
MESH = pl.DeviceIdType.MESH
OFFSETS = tuple(range(-REACH, REACH + 1))


def head_norm(product, gain_row):
    lane = lax.broadcasted_iota(jnp.int32, product.shape, 1)
    squares = product * product
    scale = jnp.zeros_like(product)
    for head in range(product.shape[1] // MEM_HD):
        inside = (lane >= head * MEM_HD) & (lane < (head + 1) * MEM_HD)
        total = jnp.sum(jnp.where(inside, squares, 0.0), axis=-1, keepdims=True)
        scale = jnp.where(inside, lax.rsqrt(total * (1.0 / MEM_HD) + NORM_EPS), scale)
    return (product * scale * gain_row).astype(jnp.bfloat16)


def dot32(left, right):
    return jnp.dot(left, right, preferred_element_type=jnp.float32)


def row_norm(rows, gain_row):
    wide = rows.astype(jnp.float32)
    factor = lax.rsqrt(jnp.mean(wide * wide, axis=-1, keepdims=True) + NORM_EPS)
    return (wide * factor * gain_row).astype(jnp.bfloat16)


def split_axis(count):
    plane = 1
    for size in range(1, count + 1):
        if count % size == 0 and size * size <= count:
            plane = size
    return count // plane, plane


def layer_kernel(
    depth,
    plane,
    most,
    passes,
    slots_ref,
    wanted_smem,
    wanted_ref,
    norm_gain_ref,
    passage_gain_ref,
    key_gain_ref,
    query_gain_ref,
    ln_gain_ref,
    gate_ref,
    taps_ref,
    tokens_hbm,
    store_hbm,
    key_w_hbm,
    value_w_hbm,
    query_w_hbm,
    conv_value_hbm,
    conv_gate_hbm,
    conv_out_hbm,
    mem_out_hbm,
    keep_hbm,
    back_hbm,
    key_w,
    value_w,
    query_w,
    conv_value,
    conv_gate,
    conv_out_w,
    mem_out_w,
    store_buf,
    x_buf,
    padded,
    filtered,
    acc,
    queries,
    memory,
    stats,
    stats_in,
    part_out,
    part_keep,
    ids_in,
    ids_smem,
    slots,
    *rest,
):
    columns, rest = dict(zip(OFFSETS, rest[: len(OFFSETS)])), rest[len(OFFSETS) :]
    (
        picked,
        far_picked,
        load_sem,
        store_sem,
        x_sem,
        ids_copy_sem,
        ids_send,
        ids_recv,
        hop_send,
        hop_recv,
        plane_send,
        plane_recv,
        far_send,
        far_recv,
        tp_send,
        tp_recv,
        out_sem,
    ) = rest
    me = lax.axis_index("st")
    tp = lax.axis_index("tp")
    z, p = me // plane, me % plane
    power = plane & (plane - 1) == 0
    passage_len = slots.shape[3]
    store_size = columns[0].shape[0]
    tile_passages = store_buf.shape[1] // passage_len
    tiles = store_size // tile_passages
    tile_rows = tile_passages * passage_len
    tokens, features = x_buf.shape
    half = features // 2
    width = key_w.shape[1]

    def reader_place(step):
        return p ^ step if power else (p + step) % plane

    def asker_place(step):
        return p ^ step if power else (p - step + plane) % plane

    far_planes = [o for o in range(depth) if max(o, depth - 1 - o) > REACH]

    def is_far(other):
        return jnp.abs(other - z) > REACH

    def store_copy(tile):
        return pltpu.make_async_copy(
            store_hbm.at[pl.ds(tile * tile_rows, tile_rows)],
            store_buf.at[tile],
            store_sem.at[tile],
        )

    loads = [
        pltpu.make_async_copy(src, dst, load_sem.at[number])
        for number, (src, dst) in enumerate(
            [
                (key_w_hbm, key_w),
                (value_w_hbm, value_w),
                (query_w_hbm, query_w),
                (conv_value_hbm, conv_value),
                (conv_gate_hbm, conv_gate),
                (conv_out_hbm, conv_out_w),
                (mem_out_hbm, mem_out_w),
            ]
        )
    ]
    mine = pl.ds(pl.multiple_of(tp * half, half), half)
    x_copy = pltpu.make_async_copy(tokens_hbm, x_buf.at[:, mine], x_sem)
    store_copy(0).start()
    loads[0].start()
    loads[1].start()
    for tile in range(1, tiles):
        store_copy(tile).start()
    x_copy.start()
    for load in loads[2:]:
        load.start()

    barrier = pltpu.get_barrier_semaphore()

    def greet(st, core):
        pl.semaphore_signal(barrier, inc=1, device_id=(st, core), device_id_type=MESH)

    greet(me, 1 - tp)
    for step in range(1, plane):
        greet(z * plane + reader_place(step), tp)

    @pl.when(z > 0)
    def _():
        greet(me - plane, tp)

    @pl.when(z < depth - 1)
    def _():
        greet(me + plane, tp)

    met = 1 + plane - 1 + jnp.where(z > 0, 1, 0) + jnp.where(z < depth - 1, 1, 0)
    for other in far_planes:

        @pl.when(is_far(other))
        def _(other=other):
            for place in range(plane):
                greet(other * plane + place, tp)

        met = met + jnp.where(is_far(other), plane, 0)
    pl.semaphore_wait(barrier, met)

    def ids_copy(st, send_slot):
        return pltpu.make_async_remote_copy(
            src_ref=wanted_ref,
            dst_ref=ids_in.at[me],
            send_sem=ids_send.at[send_slot],
            recv_sem=ids_recv.at[me],
            device_id=(st, tp),
            device_id_type=MESH,
        )

    def ids_arrival(st):
        return pltpu.make_async_remote_copy(
            src_ref=wanted_ref,
            dst_ref=ids_in.at[st],
            send_sem=ids_send.at[st],
            recv_sem=ids_recv.at[st],
            device_id=(st, tp),
            device_id_type=MESH,
        )

    def ids_local(st):
        return pltpu.make_async_copy(ids_in.at[st], ids_smem.at[st], ids_copy_sem.at[st])

    def for_askers(action):
        for step in range(1, plane):
            action(z * plane + reader_place(step))
        for other in far_planes:

            @pl.when(is_far(other))
            def _(other=other):
                for place in range(plane):
                    action(other * plane + place)

    for_askers(lambda st: ids_copy(st, st).start())

    swap = pltpu.make_async_remote_copy(
        src_ref=tokens_hbm,
        dst_ref=x_buf.at[:, mine],
        send_sem=tp_send.at[0],
        recv_sem=tp_recv.at[0],
        device_id=(me, 1 - tp),
        device_id_type=MESH,
    )
    swap.start()

    def hop(level, up, tile):
        source = columns[-level if up else level]
        target = columns[-level - 1 if up else level + 1]
        rows = pl.ds(tile * tile_passages, tile_passages)
        return pltpu.make_async_remote_copy(
            src_ref=source.at[rows],
            dst_ref=target.at[rows],
            send_sem=hop_send.at[level, int(up), tile],
            recv_sem=hop_recv.at[level, int(up), tile],
            device_id=(me + plane if up else me - plane, tp),
            device_id_type=MESH,
        )

    def sends(level, up):
        if up:
            return (z >= level) & (z < depth - 1)
        return (z <= depth - 1 - level) & (z > 0)

    def gets(level, up):
        if up:
            return z >= level + 1
        return z <= depth - 2 - level

    def start_hop(level, tile):
        for up in (True, False):

            @pl.when(sends(level, up))
            def _(up=up):
                hop(level, up, tile).start()

    def await_hop(level, tile):
        for up in (True, False):

            @pl.when(gets(level, up))
            def _(up=up):
                hop(level, up, tile).wait_recv()

    def end_hop(level, tile):
        for up in (True, False):

            @pl.when(sends(level, up))
            def _(up=up):
                hop(level, up, tile).wait_send()

    loads[0].wait()
    loads[1].wait()

    @pl.loop(0, tiles)
    def _(tile):
        store_copy(tile).wait()
        normed = row_norm(store_buf[tile], passage_gain_ref[...].astype(jnp.float32)[None, :])
        keys = head_norm(dot32(normed, key_w[...]), key_gain_ref[...].astype(jnp.float32)[None, :])
        values = dot32(normed, value_w[...]).astype(jnp.bfloat16)
        rows = pl.ds(tile * tile_passages, tile_passages)
        columns[0][rows, :, :width] = keys.reshape(tile_passages, passage_len, width)
        columns[0][rows, :, width:] = values.reshape(tile_passages, passage_len, width)
        start_hop(0, tile)

    def take_ids(st):
        ids_arrival(st).wait_recv()
        ids_local(st).start()

    for_askers(take_ids)
    for_askers(lambda st: ids_local(st).wait())

    def plane_copy(offset, step):
        return pltpu.make_async_remote_copy(
            src_ref=picked.at[offset + REACH, step - 1],
            dst_ref=slots.at[z + offset, step],
            send_sem=plane_send.at[offset + REACH, step],
            recv_sem=plane_recv.at[offset + REACH, step],
            device_id=(z * plane + reader_place(step), tp),
            device_id_type=MESH,
        )

    def held(offset):
        return (z + offset >= 0) & (z + offset < depth)

    def deliver(offset):
        @pl.when(held(offset))
        def _():
            owner = (z + offset) * plane + p
            for step in range(plane - 1, -1, -1):
                reader = z * plane + reader_place(step)
                for rank in range(most):
                    entry = owner * most + rank
                    if step == 0:
                        index = wanted_smem[entry]
                        slots[z + offset, 0, rank] = columns[offset][index]
                    else:
                        index = ids_smem[reader, 0, entry]
                        picked[offset + REACH, step - 1, rank] = columns[offset][index]
            for step in range(plane - 1, 0, -1):
                plane_copy(offset, step).start()

    def far_row(other):
        near = jnp.minimum(z, REACH) + REACH + 1
        return jnp.where(other < z, other, jnp.maximum(other - near, 0))

    def far_copy(other, place):
        step = p ^ place if power else (place - p + plane) % plane
        return pltpu.make_async_remote_copy(
            src_ref=far_picked.at[far_row(other), place],
            dst_ref=slots.at[z, step],
            send_sem=far_send.at[other, place],
            recv_sem=far_recv.at[z, step],
            device_id=(other * plane + place, tp),
            device_id_type=MESH,
        )

    def far_arrival(other, step):
        return pltpu.make_async_remote_copy(
            src_ref=far_picked.at[far_row(other), step],
            dst_ref=slots.at[other, step],
            send_sem=far_send.at[other, step],
            recv_sem=far_recv.at[other, step],
            device_id=(other * plane + asker_place(step), tp),
            device_id_type=MESH,
        )

    def deliver_far():
        for other in far_planes:

            @pl.when(is_far(other))
            def _(other=other):
                for place in range(plane):
                    for rank in range(most):
                        index = ids_smem[other * plane + place, 0, me * most + rank]
                        far_picked[far_row(other), place, rank] = columns[0][index]
                for place in range(plane):
                    far_copy(other, place).start()

    deliver(0)

    for load in loads[2:5]:
        load.wait()
    x_copy.wait()
    swap.wait()
    taps = taps_ref.shape[0]
    lead = -(-(taps - 1) // 8) * 8
    length = tokens // SEQS_DEV
    channels = padded.shape[2]
    token_tile = min(256, length)
    per_sequence = length // token_tile
    for sequence in range(SEQS_DEV):
        padded[sequence, :lead, :] = jnp.zeros((lead, channels), jnp.float32)
        padded[sequence, lead + length :, :] = jnp.zeros((8, channels), jnp.float32)

    def project(tile):
        rows = pl.ds(pl.multiple_of(tile * token_tile, token_tile), token_tile)
        normed = row_norm(x_buf[rows, :], norm_gain_ref[...].astype(jnp.float32)[None, :])
        queries[rows, :] = head_norm(dot32(normed, query_w[...]), query_gain_ref[...].astype(jnp.float32)[None, :])
        value = dot32(normed, conv_value[...])
        gate = dot32(normed, conv_gate[...])
        gated = (value * jax.nn.sigmoid(gate)).astype(jnp.bfloat16).astype(jnp.float32)
        sequence, part = tile // per_sequence, tile % per_sequence
        start = pl.multiple_of(lead + part * token_tile, 8)
        padded[sequence, pl.ds(start, token_tile), :] = gated

    token_tiles = tokens // token_tile

    @pl.loop(0, token_tiles)
    def _(tile):
        project(tile)

        @pl.when(tile < tiles - 1)
        def _():
            await_hop(0, tile)
            start_hop(1, tile)

    chunk = 64
    span = chunk + lead + 8
    block_width = 256 if channels % 256 == 0 else channels

    def convolve(sequence):
        @pl.loop(0, length // chunk)
        def _(index):
            base = pl.multiple_of(index * chunk, chunk)
            for left in range(0, channels, block_width):
                cols = slice(left, left + block_width)
                window = padded[sequence, pl.ds(base, span), cols]
                total = jnp.zeros((chunk, block_width), jnp.float32)
                for shift in range(8):
                    moved = window if shift == 0 else pltpu.roll(window, span - shift, 0)
                    for start in range(0, lead + 1, 8):
                        tap = start + shift - (lead - taps + 1)
                        if 0 <= tap < taps:
                            weight = taps_ref[tap : tap + 1, cols].astype(jnp.float32)
                            total += weight * moved[start : start + chunk, :]
                out_rows = pl.ds(pl.multiple_of(sequence * length + base, chunk), chunk)
                filtered[out_rows, cols] = total

    convolve(0)
    for tile in range(min(token_tiles, tiles - 1), tiles):
        await_hop(0, tile)
        start_hop(1, tile)
    for distance in range(1, 2):
        deliver(-distance)
        deliver(distance)
    for sequence in range(1, SEQS_DEV):
        convolve(sequence)

    row_tile = 128

    @pl.loop(0, tokens // row_tile)
    def _(tile):
        rows = pl.ds(pl.multiple_of(tile * row_tile, row_tile), row_tile)
        block = filtered[rows, :]
        lane = lax.broadcasted_iota(jnp.int32, (row_tile, 128), 1)
        first = jnp.sum(block, axis=-1, keepdims=True)
        second = jnp.sum(block * block, axis=-1, keepdims=True)
        stats[rows, :] = jnp.where(lane == 0, first, second)

    def tp_copy(number, source, target):
        return pltpu.make_async_remote_copy(
            src_ref=source,
            dst_ref=target,
            send_sem=tp_send.at[number],
            recv_sem=tp_recv.at[number],
            device_id=(me, 1 - tp),
            device_id_type=MESH,
        )

    stats_copy = tp_copy(1, stats, stats_in)
    stats_copy.start()
    loads[5].wait()
    loads[6].wait()
    stats_copy.wait()

    @pl.loop(0, tokens // row_tile)
    def _(tile):
        rows = pl.ds(pl.multiple_of(tile * row_tile, row_tile), row_tile)
        sums = stats[rows, :] + stats_in[rows, :]
        mean = sums[:, 0:1] / C_A
        variance = sums[:, 1:2] / C_A - mean * mean
        scaled = (
            (filtered[rows, :] - mean)
            * lax.rsqrt(variance + LAYER_EPS)
            * ln_gain_ref[...].astype(jnp.float32)[None, :]
        )
        acc[rows, :] = dot32(jax.nn.silu(scaled).astype(jnp.bfloat16), conv_out_w[...])

    for tile in range(tiles):
        await_hop(1, tile)
    for distance in range(2, REACH + 1):
        deliver(-distance)
        deliver(distance)
    deliver_far()
    for offset in OFFSETS:

        @pl.when(held(offset))
        def _(offset=offset):
            for step in range(1, plane):
                plane_copy(offset, step).wait_recv()

    for other in far_planes:

        @pl.when(is_far(other))
        def _(other=other):
            for step in range(plane):
                far_arrival(other, step).wait_recv()

    heads = width // MEM_HD
    blocks = slots_ref.shape[0] // passes
    block = tokens // blocks
    head_of = lax.broadcasted_iota(jnp.int32, (heads * block, width), 1) // MEM_HD
    row_head = lax.broadcasted_iota(jnp.int32, (heads * block, width), 0) // block
    inside = head_of == row_head
    gate = jnp.tanh(gate_ref[...].astype(jnp.float32)[None, :])

    def attend(first, count):
        @pl.loop(0, count, unroll=4 if count % 4 == 0 else 1)
        def _(number):
            index = first + number
            rows = pl.ds(pl.multiple_of(index * block, block), block)
            query = queries[rows, :]
            stacked = jnp.concatenate([query] * heads, axis=0)
            stacked = jnp.where(inside, stacked, jnp.zeros_like(stacked))
            read = []
            for part in range(passes):
                slot = slots_ref[index * passes + part]
                read.append(slots[slot // (plane * most), slot // most % plane, slot % most])
            keys = jnp.concatenate([part[:, :width] for part in read], axis=0)
            values = jnp.concatenate([part[:, width:] for part in read], axis=0)
            scores = lax.dot_general(
                stacked, keys, (((1,), (1,)), ((), ())), preferred_element_type=jnp.float32
            ) * MEM_HD ** (-0.5)
            expanded = jnp.exp(scores - jnp.max(scores, axis=-1, keepdims=True))
            weights = (expanded / jnp.sum(expanded, axis=-1, keepdims=True)).astype(jnp.bfloat16)
            mixed = jnp.where(inside, dot32(weights, values), 0.0)
            attended = mixed[:block]
            for head in range(1, heads):
                attended = attended + mixed[head * block : (head + 1) * block]
            memory[rows, :] = (attended * gate).astype(jnp.bfloat16)

    share = tokens // 2
    pieces = part_out.shape[0]
    piece = share // pieces
    theirs, ours = (1 - tp) * share, tp * share
    attend((1 - tp) * (blocks // 2), blocks // 2)
    part_copies = [
        tp_copy(2 + n, part_out.at[n], back_hbm.at[pl.ds(n * piece, piece)])
        for n in range(pieces)
    ]
    for number in range(pieces):
        rows = pl.ds(pl.multiple_of(theirs + number * piece, piece), piece)
        part_out[number] = (acc[rows, :] + dot32(memory[rows, :], mem_out_w[...])).astype(
            jnp.bfloat16
        )
        part_copies[number].start()
    attend(tp * (blocks // 2), blocks // 2)
    out_copies = [
        pltpu.make_async_copy(
            part_keep.at[n], keep_hbm.at[pl.ds(n * piece, piece)], out_sem.at[n]
        )
        for n in range(pieces)
    ]
    for number in range(pieces):
        rows = pl.ds(pl.multiple_of(ours + number * piece, piece), piece)
        part_keep[number] = (acc[rows, :] + dot32(memory[rows, :], mem_out_w[...])).astype(
            jnp.bfloat16
        )
        out_copies[number].start()

    for_askers(lambda st: ids_copy(st, st).wait_send())
    for level in range(REACH):
        for tile in range(tiles):
            end_hop(level, tile)
    for offset in OFFSETS:

        @pl.when(held(offset))
        def _(offset=offset):
            for step in range(1, plane):
                plane_copy(offset, step).wait_send()

    for other in far_planes:

        @pl.when(is_far(other))
        def _(other=other):
            for place in range(plane):
                far_copy(other, place).wait_send()

    for copy in part_copies + out_copies:
        copy.wait()


def add_kernel(keep_ref, back_ref, out_ref):
    out_ref[...] = (
        keep_ref[...].astype(jnp.float32) + back_ref[...].astype(jnp.float32)
    ).astype(jnp.bfloat16)


def add_parts(keep, back):
    rows, features = keep.shape
    tile = min(128, rows)
    spec = pl.BlockSpec((tile, features), lambda i: (i, 0))
    return pl.pallas_call(
        add_kernel,
        grid=(rows // tile,),
        in_specs=[spec, spec],
        out_specs=spec,
        out_shape=jax.ShapeDtypeStruct(keep.shape, jnp.bfloat16),
        compiler_params=pltpu.CompilerParams(dimension_semantics=("arbitrary",)),
        name="add_parts",
    )(keep, back)


def layer(
    tokens,
    passage_ids,
    passage_store,
    norm_gain,
    conv_value_weight,
    conv_gate_weight,
    conv_weight,
    ln_gain,
    query_weight,
    query_gain,
    passage_gain,
    key_weight,
    value_weight,
    key_gain,
    memory_gate,
    conv_out_weight,
    memory_out_weight,
):
    owner_count = lax.axis_size("st")
    me = lax.axis_index("st").astype(jnp.int32)
    depth, plane = split_axis(owner_count)
    power = plane & (plane - 1) == 0
    store_size, passage_len, features = passage_store.shape
    count, _ = tokens.shape
    width = key_weight.shape[1]
    channels = conv_weight.shape[1]

    flat_ids = passage_ids.reshape(-1)
    request_count = flat_ids.shape[0]
    most = max(1, 2 * request_count // owner_count)
    owner_index = flat_ids // store_size
    local_index = flat_ids % store_size
    same = (owner_index[:, None] == owner_index[None, :]) & (
        jnp.arange(request_count)[:, None] > jnp.arange(request_count)[None, :]
    )
    rank = jnp.sum(same.astype(jnp.int32), axis=1)
    place, my_place = owner_index % plane, me % plane
    step_to = (place ^ my_place) if power else (my_place - place + plane) % plane
    slot_index = ((owner_index // plane) * plane + step_to) * most + rank
    entry = owner_index * most + rank
    wide = -(-owner_count * most // 128) * 128
    onehot = (entry[:, None] == jnp.arange(wide, dtype=jnp.int32)[None, :]).astype(jnp.int32)
    wanted = jnp.sum(onehot * local_index[:, None], axis=0)

    tile_passages = max(1, min(256 // passage_len, store_size))
    tiles = store_size // tile_passages
    lead = -(-(conv_weight.shape[0] - 1) // 8) * 8
    length = count // SEQS_DEV
    share = count // 2
    pieces = 2
    row = (passage_len, 2 * width)
    bf16, f32 = jnp.bfloat16, jnp.float32
    vmem = pl.BlockSpec(memory_space=pltpu.VMEM)
    smem = pl.BlockSpec(memory_space=pltpu.SMEM)
    anywhere = pl.BlockSpec(memory_space=pl.ANY)
    dma = pltpu.SemaphoreType.DMA
    weights = (
        key_weight,
        value_weight,
        query_weight,
        conv_value_weight,
        conv_gate_weight,
        conv_out_weight,
        memory_out_weight,
    )
    reach = len(OFFSETS)
    scratch = (
        [pltpu.VMEM(w.shape, bf16) for w in weights]
        + [
            pltpu.VMEM((tiles, tile_passages * passage_len, features), bf16),
            pltpu.VMEM((count, features), bf16),
            pltpu.VMEM((SEQS_DEV, lead + length + 8, channels), f32),
            pltpu.VMEM((count, channels), f32),
            pltpu.VMEM((count, features), f32),
            pltpu.VMEM((count, width), bf16),
            pltpu.VMEM((count, width), bf16),
            pltpu.VMEM((count, 128), f32),
            pltpu.VMEM((count, 128), f32),
            pltpu.VMEM((pieces, share // pieces, features), bf16),
            pltpu.VMEM((pieces, share // pieces, features), bf16),
            pltpu.VMEM((owner_count, 1, wide), jnp.int32),
            pltpu.SMEM((owner_count, 1, wide), jnp.int32),
            pltpu.VMEM((depth, plane, most) + row, bf16),
        ]
        + [pltpu.VMEM((store_size,) + row, bf16) for _ in OFFSETS]
        + [
            pltpu.VMEM((reach, max(plane - 1, 1), most) + row, bf16),
            pltpu.VMEM((max(depth - 1 - REACH, 1), plane, most) + row, bf16),
            dma((len(weights),)),
            dma((tiles,)),
            dma,
            dma((owner_count,)),
            dma((owner_count,)),
            dma((owner_count,)),
            dma((REACH, 2, tiles)),
            dma((REACH, 2, tiles)),
            dma((reach, plane)),
            dma((reach, plane)),
            dma((depth, plane)),
            dma((depth, plane)),
            dma((2 + pieces,)),
            dma((2 + pieces,)),
            dma((pieces,)),
        ]
    )
    keep, back = pl.pallas_call(
        functools.partial(layer_kernel, depth, plane, most, passage_ids.shape[1]),
        in_specs=[smem, smem] + [vmem] * 8 + [anywhere] * (2 + len(weights)),
        out_specs=[anywhere] * 2,
        out_shape=[jax.ShapeDtypeStruct((share, features), bf16)] * 2,
        scratch_shapes=scratch,
        compiler_params=pltpu.CompilerParams(
            collective_id=0, has_side_effects=True, vmem_limit_bytes=67043328
        ),
        cost_estimate=pl.CostEstimate(
            flops=16 << 30, bytes_accessed=24 << 20, transcendentals=0
        ),
        name="layer",
    )(
        slot_index,
        wanted,
        wanted[None, :],
        norm_gain,
        passage_gain,
        key_gain,
        query_gain,
        ln_gain,
        memory_gate,
        conv_weight,
        tokens,
        passage_store.reshape(-1, features),
        *weights,
    )
    return add_parts(keep, back)


def solution(mesh):
    return jax.shard_map(
        layer,
        mesh=mesh,
        in_specs=(
            P("st", "tp"),
            P("st", None),
            P("st", None, None),
            P(),
            P(None, "tp"),
            P(None, "tp"),
            P(None, "tp"),
            P("tp"),
            P(None, "tp"),
            P("tp"),
            P(),
            P(None, "tp"),
            P(None, "tp"),
            P("tp"),
            P("tp"),
            P("tp", None),
            P("tp", None),
        ),
        out_specs=P(("st", "tp"), None),
        check_vma=False,
    )
```

```python
import functools

import jax
import jax.numpy as jnp
from jax import lax
from jax.experimental import pallas as pl
from jax.experimental.pallas import tpu as pltpu
from jax.sharding import PartitionSpec as P

C_A = 1536
MEM_HD = 64
SEQS_DEV = 2
NORM_EPS = 1e-06
LAYER_EPS = 1e-05
REACH = 2
MESH = pl.DeviceIdType.MESH
OFFSETS = tuple(range(-REACH, REACH + 1))


def head_norm(product, gain_row):
    lane = lax.broadcasted_iota(jnp.int32, product.shape, 1)
    squares = product * product
    scale = jnp.zeros_like(product)
    for head in range(product.shape[1] // MEM_HD):
        inside = (lane >= head * MEM_HD) & (lane < (head + 1) * MEM_HD)
        total = jnp.sum(jnp.where(inside, squares, 0.0), axis=-1, keepdims=True)
        scale = jnp.where(inside, lax.rsqrt(total * (1.0 / MEM_HD) + NORM_EPS), scale)
    return (product * scale * gain_row).astype(jnp.bfloat16)


def dot32(left, right):
    return jnp.dot(left, right, preferred_element_type=jnp.float32)


def row_norm(rows, gain_row):
    wide = rows.astype(jnp.float32)
    factor = lax.rsqrt(jnp.mean(wide * wide, axis=-1, keepdims=True) + NORM_EPS)
    return (wide * factor * gain_row).astype(jnp.bfloat16)


def split_axis(count):
    plane = 1
    for size in range(1, count + 1):
        if count % size == 0 and size * size <= count:
            plane = size
    return count // plane, plane


def layer_kernel(
    depth,
    plane,
    most,
    passes,
    ids_ref,
    norm_gain_ref,
    passage_gain_ref,
    key_gain_ref,
    query_gain_ref,
    ln_gain_ref,
    gate_ref,
    taps_ref,
    tokens_hbm,
    store_hbm,
    key_w_hbm,
    value_w_hbm,
    query_w_hbm,
    conv_value_hbm,
    conv_gate_hbm,
    conv_out_hbm,
    mem_out_hbm,
    keep_ref,
    back_ref,
    key_w,
    value_w,
    query_w,
    conv_value,
    conv_gate,
    conv_out_w,
    mem_out_w,
    store_buf,
    x_buf,
    padded,
    filtered,
    acc,
    queries,
    memory,
    stats,
    stats_in,
    wanted_ref,
    wanted_smem,
    slots_ref,
    ids_in,
    ids_smem,
    slots,
    *rest,
):
    columns, rest = dict(zip(OFFSETS, rest[: len(OFFSETS)])), rest[len(OFFSETS) :]
    (
        picked,
        far_picked,
        far_stage,
        load_sem,
        store_sem,
        x_sem,
        wanted_sem,
        ids_copy_sem,
        ids_send,
        ids_recv,
        hop_send,
        hop_recv,
        plane_send,
        plane_recv,
        stage_send,
        stage_recv,
        far_send,
        far_recv,
        tp_send,
        tp_recv,
    ) = rest
    me = lax.axis_index("st")
    tp = lax.axis_index("tp")
    z, p = me // plane, me % plane
    power = plane & (plane - 1) == 0
    passage_len = slots.shape[3]
    store_size = columns[0].shape[0]
    tile_passages = store_buf.shape[1] // passage_len
    tiles = store_size // tile_passages
    tile_rows = tile_passages * passage_len
    tokens, features = x_buf.shape
    half = features // 2
    width = key_w.shape[1]

    def reader_place(step):
        return p ^ step if power else (p + step) % plane

    far_planes = [o for o in range(depth) if max(o, depth - 1 - o) > REACH]

    def is_far(other):
        return jnp.abs(other - z) > REACH

    def store_copy(tile):
        return pltpu.make_async_copy(
            store_hbm.at[pl.ds(tile * tile_rows, tile_rows)],
            store_buf.at[tile],
            store_sem.at[tile],
        )

    loads = [
        pltpu.make_async_copy(src, dst, load_sem.at[number])
        for number, (src, dst) in enumerate(
            [
                (key_w_hbm, key_w),
                (value_w_hbm, value_w),
                (query_w_hbm, query_w),
                (conv_value_hbm, conv_value),
                (conv_gate_hbm, conv_gate),
                (conv_out_hbm, conv_out_w),
                (mem_out_hbm, mem_out_w),
            ]
        )
    ]
    mine = pl.ds(pl.multiple_of(tp * half, half), half)
    x_copy = pltpu.make_async_copy(tokens_hbm, x_buf.at[:, mine], x_sem)
    store_copy(0).start()
    loads[0].start()
    loads[1].start()
    barrier = pltpu.get_barrier_semaphore()

    def greet(st, core):
        pl.semaphore_signal(barrier, inc=1, device_id=(st, core), device_id_type=MESH)

    greet(me, 1 - tp)
    for step in range(1, plane):
        greet(z * plane + reader_place(step), tp)

    @pl.when(z > 0)
    def _():
        greet(me - plane, tp)

    @pl.when(z < depth - 1)
    def _():
        greet(me + plane, tp)

    met = 1 + plane - 1 + jnp.where(z > 0, 1, 0) + jnp.where(z < depth - 1, 1, 0)
    for other in far_planes:

        @pl.when(is_far(other))
        def _(other=other):
            for place in range(plane):
                greet(other * plane + place, tp)

        met = met + jnp.where(is_far(other), plane, 0)

    requests = slots_ref.shape[0]
    owners, rows_asked = [], []
    for number in range(requests):
        asked = ids_ref[number % passes, number // passes]
        owners.append(lax.div(asked, store_size))
        rows_asked.append(lax.rem(asked, store_size))
    lane = lax.broadcasted_iota(jnp.int32, wanted_ref.shape, 1)
    wanted = jnp.zeros(wanted_ref.shape, jnp.int32)
    for number, owner in enumerate(owners):
        rank = jnp.int32(0)
        for before in owners[:number]:
            rank = rank + (before == owner).astype(jnp.int32)
        place = lax.rem(owner, plane)
        step = place ^ p if power else lax.rem(p - place + plane, plane)
        slots_ref[number] = (lax.div(owner, plane) * plane + step) * most + rank
        wanted = wanted + jnp.where(lane == owner * most + rank, rows_asked[number], 0)
    wanted_ref[...] = wanted
    own_ids = pltpu.make_async_copy(wanted_ref, wanted_smem, wanted_sem)

    def project_passages(tile):
        normed = row_norm(store_buf[tile], passage_gain_ref[...].astype(jnp.float32)[None, :])
        keys = head_norm(dot32(normed, key_w[...]), key_gain_ref[...].astype(jnp.float32)[None, :])
        values = dot32(normed, value_w[...]).astype(jnp.bfloat16)
        rows = pl.ds(tile * tile_passages, tile_passages)
        columns[0][rows, :, :width] = keys.reshape(tile_passages, passage_len, width)
        columns[0][rows, :, width:] = values.reshape(tile_passages, passage_len, width)

    loads[0].wait()
    loads[1].wait()
    store_copy(0).wait()
    for tile in range(1, tiles):
        store_copy(tile).start()
    x_copy.start()
    for load in loads[2:]:
        load.start()
    project_passages(0)
    pl.semaphore_wait(barrier, met)

    def ids_copy(st, send_slot):
        return pltpu.make_async_remote_copy(
            src_ref=wanted_ref,
            dst_ref=ids_in.at[me],
            send_sem=ids_send.at[send_slot],
            recv_sem=ids_recv.at[me],
            device_id=(st, tp),
            device_id_type=MESH,
        )

    def ids_arrival(st):
        return pltpu.make_async_remote_copy(
            src_ref=wanted_ref,
            dst_ref=ids_in.at[st],
            send_sem=ids_send.at[st],
            recv_sem=ids_recv.at[st],
            device_id=(st, tp),
            device_id_type=MESH,
        )

    def ids_local(st):
        return pltpu.make_async_copy(ids_in.at[st], ids_smem.at[st], ids_copy_sem.at[st])

    def for_askers(action):
        for step in range(1, plane):
            action(z * plane + reader_place(step))
        for other in far_planes:

            @pl.when(is_far(other))
            def _(other=other):
                for place in range(plane):
                    action(other * plane + place)

    def hop(level, up, tile):
        source = columns[-level if up else level]
        target = columns[-level - 1 if up else level + 1]
        rows = pl.ds(tile * tile_passages, tile_passages)
        return pltpu.make_async_remote_copy(
            src_ref=source.at[rows],
            dst_ref=target.at[rows],
            send_sem=hop_send.at[level, int(up), tile],
            recv_sem=hop_recv.at[level, int(up), tile],
            device_id=(me + plane if up else me - plane, tp),
            device_id_type=MESH,
        )

    def sends(level, up):
        if up:
            return (z >= level) & (z < depth - 1)
        return (z <= depth - 1 - level) & (z > 0)

    def gets(level, up):
        if up:
            return z >= level + 1
        return z <= depth - 2 - level

    def start_hop(level, tile):
        for up in (True, False):

            @pl.when(sends(level, up))
            def _(up=up):
                hop(level, up, tile).start()

    def await_hop(level, tile):
        for up in (True, False):

            @pl.when(gets(level, up))
            def _(up=up):
                hop(level, up, tile).wait_recv()

    def end_hop(level, tile):
        for up in (True, False):

            @pl.when(sends(level, up))
            def _(up=up):
                hop(level, up, tile).wait_send()

    own_ids.start()
    for_askers(lambda st: ids_copy(st, st).start())
    start_hop(0, 0)

    swap = pltpu.make_async_remote_copy(
        src_ref=tokens_hbm,
        dst_ref=x_buf.at[:, mine],
        send_sem=tp_send.at[0],
        recv_sem=tp_recv.at[0],
        device_id=(me, 1 - tp),
        device_id_type=MESH,
    )
    swap.start()

    @pl.loop(1, tiles)
    def _(tile):
        store_copy(tile).wait()
        project_passages(tile)
        start_hop(0, tile)

    def take_ids(st):
        ids_arrival(st).wait_recv()
        ids_local(st).start()

    for_askers(take_ids)
    for_askers(lambda st: ids_local(st).wait())
    own_ids.wait()

    def plane_copy(offset, step):
        return pltpu.make_async_remote_copy(
            src_ref=picked.at[offset + REACH, step - 1],
            dst_ref=slots.at[z + offset, step],
            send_sem=plane_send.at[offset + REACH, step],
            recv_sem=plane_recv.at[offset + REACH, step],
            device_id=(z * plane + reader_place(step), tp),
            device_id_type=MESH,
        )

    def held(offset):
        return (z + offset >= 0) & (z + offset < depth)

    def deliver(offset):
        @pl.when(held(offset))
        def _():
            owner = (z + offset) * plane + p
            for step in range(plane - 1, -1, -1):
                reader = z * plane + reader_place(step)
                for rank in range(most):
                    entry = owner * most + rank
                    if step == 0:
                        index = wanted_smem[0, entry]
                        slots[z + offset, 0, rank] = columns[offset][index]
                    else:
                        index = ids_smem[reader, 0, entry]
                        picked[offset + REACH, step - 1, rank] = columns[offset][index]
            for step in range(plane - 1, 0, -1):
                plane_copy(offset, step).start()

    def far_row(other):
        near = jnp.minimum(z, REACH) + REACH + 1
        return jnp.where(other < z, other, jnp.maximum(other - near, 0))

    def stage_copy(other, step):
        return pltpu.make_async_remote_copy(
            src_ref=far_picked.at[far_row(other), step - 1],
            dst_ref=far_stage.at[far_row(other), step],
            send_sem=stage_send.at[far_row(other), step],
            recv_sem=stage_recv.at[far_row(other), step],
            device_id=(z * plane + reader_place(step), tp),
            device_id_type=MESH,
        )

    def far_copy(other, source):
        return pltpu.make_async_remote_copy(
            src_ref=far_stage.at[far_row(other)],
            dst_ref=slots.at[source],
            send_sem=far_send.at[other],
            recv_sem=far_recv.at[source],
            device_id=(other * plane + p, tp),
            device_id_type=MESH,
        )

    def for_far(action):
        for other in far_planes:

            @pl.when(is_far(other))
            def _(other=other):
                action(other)

    def stage_far(other):
        for step in range(plane - 1, -1, -1):
            reader = other * plane + reader_place(step)
            for rank in range(most):
                block = columns[0][ids_smem[reader, 0, me * most + rank]]
                if step == 0:
                    far_stage[far_row(other), 0, rank] = block
                else:
                    far_picked[far_row(other), step - 1, rank] = block
        for step in range(plane - 1, 0, -1):
            stage_copy(other, step).start()

    def send_far(other):
        for step in range(1, plane):
            stage_copy(other, step).wait_recv()
        far_copy(other, z).start()

    deliver(0)
    for_far(stage_far)

    for load in loads[2:5]:
        load.wait()
    x_copy.wait()
    swap.wait()
    taps = taps_ref.shape[0]
    lead = -(-(taps - 1) // 8) * 8
    length = tokens // SEQS_DEV
    channels = padded.shape[2]
    token_tile = min(256, length)
    per_sequence = length // token_tile
    for sequence in range(SEQS_DEV):
        padded[sequence, :lead, :] = jnp.zeros((lead, channels), jnp.float32)
        padded[sequence, lead + length :, :] = jnp.zeros((8, channels), jnp.float32)

    def project(tile):
        rows = pl.ds(pl.multiple_of(tile * token_tile, token_tile), token_tile)
        normed = row_norm(x_buf[rows, :], norm_gain_ref[...].astype(jnp.float32)[None, :])
        queries[rows, :] = head_norm(dot32(normed, query_w[...]), query_gain_ref[...].astype(jnp.float32)[None, :])
        value = dot32(normed, conv_value[...])
        gate = dot32(normed, conv_gate[...])
        gated = (value * jax.nn.sigmoid(gate)).astype(jnp.bfloat16).astype(jnp.float32)
        sequence, part = tile // per_sequence, tile % per_sequence
        start = pl.multiple_of(lead + part * token_tile, 8)
        padded[sequence, pl.ds(start, token_tile), :] = gated

    token_tiles = tokens // token_tile

    @pl.loop(0, token_tiles)
    def _(tile):
        project(tile)

        @pl.when(tile < tiles - 1)
        def _():
            await_hop(0, tile)
            start_hop(1, tile)

    chunk = 64
    span = chunk + lead + 8
    block_width = 256 if channels % 256 == 0 else channels

    def convolve(sequence):
        @pl.loop(0, length // chunk)
        def _(index):
            base = pl.multiple_of(index * chunk, chunk)
            for left in range(0, channels, block_width):
                cols = slice(left, left + block_width)
                window = padded[sequence, pl.ds(base, span), cols]
                total = jnp.zeros((chunk, block_width), jnp.float32)
                for shift in range(8):
                    moved = window if shift == 0 else pltpu.roll(window, span - shift, 0)
                    for start in range(0, lead + 1, 8):
                        tap = start + shift - (lead - taps + 1)
                        if 0 <= tap < taps:
                            weight = taps_ref[tap : tap + 1, cols].astype(jnp.float32)
                            total += weight * moved[start : start + chunk, :]
                out_rows = pl.ds(pl.multiple_of(sequence * length + base, chunk), chunk)
                filtered[out_rows, cols] = total

    convolve(0)
    for tile in range(min(token_tiles, tiles - 1), tiles):
        await_hop(0, tile)
        start_hop(1, tile)
    for distance in range(1, 2):
        deliver(-distance)
        deliver(distance)
    for sequence in range(1, SEQS_DEV):
        convolve(sequence)

    row_tile = 128

    @pl.loop(0, tokens // row_tile)
    def _(tile):
        rows = pl.ds(pl.multiple_of(tile * row_tile, row_tile), row_tile)
        block = filtered[rows, :]
        lane = lax.broadcasted_iota(jnp.int32, (row_tile, 128), 1)
        first = jnp.sum(block, axis=-1, keepdims=True)
        second = jnp.sum(block * block, axis=-1, keepdims=True)
        stats[rows, :] = jnp.where(lane == 0, first, second)

    def tp_copy(number, source, target):
        return pltpu.make_async_remote_copy(
            src_ref=source,
            dst_ref=target,
            send_sem=tp_send.at[number],
            recv_sem=tp_recv.at[number],
            device_id=(me, 1 - tp),
            device_id_type=MESH,
        )

    stats_copy = tp_copy(1, stats, stats_in)
    stats_copy.start()
    loads[5].wait()
    loads[6].wait()
    stats_copy.wait()

    @pl.loop(0, tokens // row_tile)
    def _(tile):
        rows = pl.ds(pl.multiple_of(tile * row_tile, row_tile), row_tile)
        sums = stats[rows, :] + stats_in[rows, :]
        mean = sums[:, 0:1] / C_A
        variance = sums[:, 1:2] / C_A - mean * mean
        scaled = (
            (filtered[rows, :] - mean)
            * lax.rsqrt(variance + LAYER_EPS)
            * ln_gain_ref[...].astype(jnp.float32)[None, :]
        )
        acc[rows, :] = dot32(jax.nn.silu(scaled).astype(jnp.bfloat16), conv_out_w[...])

    for tile in range(tiles):
        await_hop(1, tile)
    for distance in range(2, REACH + 1):
        deliver(-distance)
        deliver(distance)
    for_far(send_far)
    for offset in OFFSETS:

        @pl.when(held(offset))
        def _(offset=offset):
            for step in range(1, plane):
                plane_copy(offset, step).wait_recv()

    for_far(lambda other: far_copy(other, other).wait_recv())

    heads = width // MEM_HD
    blocks = slots_ref.shape[0] // passes
    block = tokens // blocks
    head_of = lax.broadcasted_iota(jnp.int32, (heads * block, width), 1) // MEM_HD
    row_head = lax.broadcasted_iota(jnp.int32, (heads * block, width), 0) // block
    inside = head_of == row_head
    gate = jnp.tanh(gate_ref[...].astype(jnp.float32)[None, :])

    def attend(first, count):
        @pl.loop(0, count, unroll=4 if count % 4 == 0 else 1)
        def _(number):
            index = first + number
            rows = pl.ds(pl.multiple_of(index * block, block), block)
            query = queries[rows, :]
            stacked = jnp.concatenate([query] * heads, axis=0)
            stacked = jnp.where(inside, stacked, jnp.zeros_like(stacked))
            read = []
            for part in range(passes):
                slot = slots_ref[index * passes + part]
                read.append(slots[slot // (plane * most), slot // most % plane, slot % most])
            keys = jnp.concatenate([part[:, :width] for part in read], axis=0)
            values = jnp.concatenate([part[:, width:] for part in read], axis=0)
            scores = lax.dot_general(
                stacked, keys, (((1,), (1,)), ((), ())), preferred_element_type=jnp.float32
            ) * MEM_HD ** (-0.5)
            expanded = jnp.exp(scores - jnp.max(scores, axis=-1, keepdims=True))
            weights = (expanded / jnp.sum(expanded, axis=-1, keepdims=True)).astype(jnp.bfloat16)
            mixed = jnp.where(inside, dot32(weights, values), 0.0)
            attended = mixed[:block]
            for head in range(1, heads):
                attended = attended + mixed[head * block : (head + 1) * block]
            memory[rows, :] = (attended * gate).astype(jnp.bfloat16)

    share = tokens // 2
    pieces = tp_send.shape[0] - 2
    piece, few = share // pieces, blocks // 2 // pieces

    def part_copy(number):
        rows = pl.ds(pl.multiple_of(number * piece, piece), piece)
        return tp_copy(2 + number, x_buf.at[rows], back_ref.at[rows])

    def part_of(core, number):
        attend(core * (blocks // 2) + number * few, few)
        rows = pl.ds(pl.multiple_of(core * share + number * piece, piece), piece)
        return (acc[rows, :] + dot32(memory[rows, :], mem_out_w[...])).astype(jnp.bfloat16)

    @pl.loop(0, pieces)
    def _(number):
        x_buf[pl.ds(pl.multiple_of(number * piece, piece), piece), :] = part_of(1 - tp, number)
        part_copy(number).start()

    @pl.loop(0, pieces)
    def _(number):
        keep_ref[pl.ds(pl.multiple_of(number * piece, piece), piece), :] = part_of(tp, number)

    for_askers(lambda st: ids_copy(st, st).wait_send())
    for level in range(REACH):
        for tile in range(tiles):
            end_hop(level, tile)
    for offset in OFFSETS:

        @pl.when(held(offset))
        def _(offset=offset):
            for step in range(1, plane):
                plane_copy(offset, step).wait_send()

    def end_far(other):
        for step in range(1, plane):
            stage_copy(other, step).wait_send()
        far_copy(other, z).wait_send()

    for_far(end_far)
    for number in range(pieces):
        part_copy(number).wait()


def add_kernel(keep_ref, back_ref, out_hbm, result, sems):
    pieces, piece = result.shape[:2]
    copies = []
    for number in range(pieces):
        rows = pl.ds(number * piece, piece)
        result[number] = (
            keep_ref[rows, :].astype(jnp.float32) + back_ref[rows, :].astype(jnp.float32)
        ).astype(jnp.bfloat16)
        copies.append(
            pltpu.make_async_copy(result.at[number], out_hbm.at[rows], sems.at[number])
        )
        copies[-1].start()
    for copy in copies:
        copy.wait()


def add_parts(keep, back):
    rows, features = keep.shape
    pieces = 4
    vmem = pl.BlockSpec(memory_space=pltpu.VMEM)
    return pl.pallas_call(
        add_kernel,
        in_specs=[vmem, vmem],
        out_specs=pl.BlockSpec(memory_space=pl.ANY),
        out_shape=jax.ShapeDtypeStruct(keep.shape, jnp.bfloat16),
        scratch_shapes=[
            pltpu.VMEM((pieces, rows // pieces, features), jnp.bfloat16),
            pltpu.SemaphoreType.DMA((pieces,)),
        ],
        compiler_params=pltpu.CompilerParams(vmem_limit_bytes=16 << 20),
        name="add_parts",
    )(keep, back)


def layer(
    tokens,
    passage_ids,
    passage_store,
    norm_gain,
    conv_value_weight,
    conv_gate_weight,
    conv_weight,
    ln_gain,
    query_weight,
    query_gain,
    passage_gain,
    key_weight,
    value_weight,
    key_gain,
    memory_gate,
    conv_out_weight,
    memory_out_weight,
):
    owner_count = lax.axis_size("st")
    depth, plane = split_axis(owner_count)
    store_size, passage_len, features = passage_store.shape
    count, _ = tokens.shape
    width = key_weight.shape[1]
    channels = conv_weight.shape[1]

    request_count = passage_ids.shape[0] * passage_ids.shape[1]
    most = max(1, 2 * request_count // owner_count)
    wide = -(-owner_count * most // 128) * 128

    tile_passages = max(1, min(256 // passage_len, store_size))
    tiles = store_size // tile_passages
    lead = -(-(conv_weight.shape[0] - 1) // 8) * 8
    length = count // SEQS_DEV
    share = count // 2
    pieces = 2
    row = (passage_len, 2 * width)
    bf16, f32 = jnp.bfloat16, jnp.float32
    vmem = pl.BlockSpec(memory_space=pltpu.VMEM)
    smem = pl.BlockSpec(memory_space=pltpu.SMEM)
    anywhere = pl.BlockSpec(memory_space=pl.ANY)
    dma = pltpu.SemaphoreType.DMA
    weights = (
        key_weight,
        value_weight,
        query_weight,
        conv_value_weight,
        conv_gate_weight,
        conv_out_weight,
        memory_out_weight,
    )
    reach = len(OFFSETS)
    far_rows = max(depth - 1 - REACH, 1)
    scratch = (
        [pltpu.VMEM(w.shape, bf16) for w in weights]
        + [
            pltpu.VMEM((tiles, tile_passages * passage_len, features), bf16),
            pltpu.VMEM((count, features), bf16),
            pltpu.VMEM((SEQS_DEV, lead + length + 8, channels), f32),
            pltpu.VMEM((count, channels), f32),
            pltpu.VMEM((count, features), f32),
            pltpu.VMEM((count, width), bf16),
            pltpu.VMEM((count, width), bf16),
            pltpu.VMEM((count, 128), f32),
            pltpu.VMEM((count, 128), f32),
            pltpu.VMEM((1, wide), jnp.int32),
            pltpu.SMEM((1, wide), jnp.int32),
            pltpu.SMEM((request_count,), jnp.int32),
            pltpu.VMEM((owner_count, 1, wide), jnp.int32),
            pltpu.SMEM((owner_count, 1, wide), jnp.int32),
            pltpu.VMEM((depth, plane, most) + row, bf16),
        ]
        + [pltpu.VMEM((store_size,) + row, bf16) for _ in OFFSETS]
        + [
            pltpu.VMEM((reach, max(plane - 1, 1), most) + row, bf16),
            pltpu.VMEM((far_rows, max(plane - 1, 1), most) + row, bf16),
            pltpu.VMEM((far_rows, plane, most) + row, bf16),
            dma((len(weights),)),
            dma((tiles,)),
            dma,
            dma,
            dma((owner_count,)),
            dma((owner_count,)),
            dma((owner_count,)),
            dma((REACH, 2, tiles)),
            dma((REACH, 2, tiles)),
            dma((reach, plane)),
            dma((reach, plane)),
            dma((far_rows, plane)),
            dma((far_rows, plane)),
            dma((depth,)),
            dma((depth,)),
            dma((2 + pieces,)),
            dma((2 + pieces,)),
        ]
    )
    keep, back = pl.pallas_call(
        functools.partial(layer_kernel, depth, plane, most, passage_ids.shape[1]),
        in_specs=[smem] + [vmem] * 7 + [anywhere] * (2 + len(weights)),
        out_specs=[vmem] * 2,
        out_shape=[pltpu.VMEM((share, features), bf16)] * 2,
        scratch_shapes=scratch,
        compiler_params=pltpu.CompilerParams(
            collective_id=0, has_side_effects=True, vmem_limit_bytes=58 << 20
        ),
        cost_estimate=pl.CostEstimate(
            flops=16 << 30, bytes_accessed=24 << 20, transcendentals=0
        ),
        name="layer",
    )(
        passage_ids.T,
        norm_gain,
        passage_gain,
        key_gain,
        query_gain,
        ln_gain,
        memory_gate,
        conv_weight,
        tokens,
        passage_store.reshape(-1, features),
        *weights,
    )
    return add_parts(keep, back)


def solution(mesh):
    return jax.shard_map(
        layer,
        mesh=mesh,
        in_specs=(
            P("st", "tp"),
            P("st", None),
            P("st", None, None),
            P(),
            P(None, "tp"),
            P(None, "tp"),
            P(None, "tp"),
            P("tp"),
            P(None, "tp"),
            P("tp"),
            P(),
            P(None, "tp"),
            P(None, "tp"),
            P("tp"),
            P("tp"),
            P("tp", None),
            P("tp", None),
        ),
        out_specs=P(("st", "tp"), None),
        check_vma=False,
    )
```

```python
import functools

import jax
import jax.numpy as jnp
from jax import lax
from jax.experimental import pallas as pl
from jax.experimental.pallas import tpu as pltpu
from jax.sharding import PartitionSpec as P

C_A = 1536
MEM_HD = 64
SEQS_DEV = 2
NORM_EPS = 1e-06
LAYER_EPS = 1e-05
REACH = 2
MESH = pl.DeviceIdType.MESH
OFFSETS = tuple(range(-REACH, REACH + 1))


def head_norm(product, gain_row):
    lane = lax.broadcasted_iota(jnp.int32, product.shape, 1)
    squares = product * product
    scale = jnp.zeros_like(product)
    for head in range(product.shape[1] // MEM_HD):
        inside = (lane >= head * MEM_HD) & (lane < (head + 1) * MEM_HD)
        total = jnp.sum(jnp.where(inside, squares, 0.0), axis=-1, keepdims=True)
        scale = jnp.where(inside, lax.rsqrt(total * (1.0 / MEM_HD) + NORM_EPS), scale)
    return (product * scale * gain_row).astype(jnp.bfloat16)


def dot32(left, right):
    return jnp.dot(left, right, preferred_element_type=jnp.float32)


def row_norm(rows, gain_row):
    wide = rows.astype(jnp.float32)
    factor = lax.rsqrt(jnp.mean(wide * wide, axis=-1, keepdims=True) + NORM_EPS)
    return (wide * factor * gain_row).astype(jnp.bfloat16)


def split_axis(count):
    plane = 1
    for size in range(1, count + 1):
        if count % size == 0 and size * size <= count:
            plane = size
    return count // plane, plane


def layer_kernel(
    depth,
    plane,
    most,
    passes,
    ids_ref,
    norm_gain_ref,
    passage_gain_ref,
    key_gain_ref,
    query_gain_ref,
    ln_gain_ref,
    gate_ref,
    taps_ref,
    tokens_hbm,
    store_hbm,
    key_w_hbm,
    value_w_hbm,
    query_w_hbm,
    conv_value_hbm,
    conv_gate_hbm,
    conv_out_hbm,
    mem_out_hbm,
    keep_ref,
    back_ref,
    key_w,
    value_w,
    query_w,
    conv_value,
    conv_gate,
    conv_out_w,
    mem_out_w,
    store_buf,
    x_buf,
    padded,
    filtered,
    acc,
    queries,
    memory,
    stats,
    stats_in,
    wanted_ref,
    wanted_smem,
    slots_ref,
    ids_in,
    ids_smem,
    slots,
    *rest,
):
    columns, rest = dict(zip(OFFSETS, rest[: len(OFFSETS)])), rest[len(OFFSETS) :]
    (
        picked,
        far_picked,
        far_stage,
        load_sem,
        store_sem,
        x_sem,
        wanted_sem,
        ids_copy_sem,
        ids_send,
        ids_recv,
        hop_send,
        hop_recv,
        plane_send,
        plane_recv,
        stage_send,
        stage_recv,
        far_send,
        far_recv,
        tp_send,
        tp_recv,
    ) = rest
    me = lax.axis_index("st")
    tp = lax.axis_index("tp")
    z, p = me // plane, me % plane
    power = plane & (plane - 1) == 0
    passage_len = slots.shape[3]
    store_size = columns[0].shape[0]
    tile_passages = store_buf.shape[1] // passage_len
    tiles = store_size // tile_passages
    tile_rows = tile_passages * passage_len
    tokens, features = x_buf.shape
    half = features // 2
    width = key_w.shape[1]

    def reader_place(step):
        return p ^ step if power else (p + step) % plane

    def asker_place(step):
        return p ^ step if power else (p - step + plane) % plane

    far_planes = [o for o in range(depth) if max(o, depth - 1 - o) > REACH]

    def is_far(other):
        return jnp.abs(other - z) > REACH

    def store_copy(tile):
        return pltpu.make_async_copy(
            store_hbm.at[pl.ds(tile * tile_rows, tile_rows)],
            store_buf.at[tile],
            store_sem.at[tile],
        )

    loads = [
        pltpu.make_async_copy(src, dst, load_sem.at[number])
        for number, (src, dst) in enumerate(
            [
                (key_w_hbm, key_w),
                (value_w_hbm, value_w),
                (query_w_hbm, query_w),
                (conv_value_hbm, conv_value),
                (conv_gate_hbm, conv_gate),
                (conv_out_hbm, conv_out_w),
                (mem_out_hbm, mem_out_w),
            ]
        )
    ]
    mine = pl.ds(pl.multiple_of(tp * half, half), half)
    x_copy = pltpu.make_async_copy(tokens_hbm, x_buf.at[:, mine], x_sem)
    store_copy(0).start()
    loads[0].start()
    loads[1].start()
    barrier = pltpu.get_barrier_semaphore()

    def greet(st, core):
        pl.semaphore_signal(barrier, inc=1, device_id=(st, core), device_id_type=MESH)

    greet(me, 1 - tp)
    for step in range(1, plane):
        greet(z * plane + reader_place(step), tp)

    @pl.when(z > 0)
    def _():
        greet(me - plane, tp)

    @pl.when(z < depth - 1)
    def _():
        greet(me + plane, tp)

    met = 1 + plane - 1 + jnp.where(z > 0, 1, 0) + jnp.where(z < depth - 1, 1, 0)
    for other in far_planes:

        @pl.when(is_far(other))
        def _(other=other):
            for place in range(plane):
                greet(other * plane + place, tp)

        met = met + jnp.where(is_far(other), plane, 0)

    requests = slots_ref.shape[0]
    owners, rows_asked = [], []
    for number in range(requests):
        asked = ids_ref[number % passes, number // passes]
        owners.append(lax.div(asked, store_size))
        rows_asked.append(lax.rem(asked, store_size))
    lane = lax.broadcasted_iota(jnp.int32, wanted_ref.shape, 1)
    wanted = jnp.zeros(wanted_ref.shape, jnp.int32)
    for number, owner in enumerate(owners):
        rank = jnp.int32(0)
        for before in owners[:number]:
            rank = rank + (before == owner).astype(jnp.int32)
        place = lax.rem(owner, plane)
        step = place ^ p if power else lax.rem(p - place + plane, plane)
        slots_ref[number] = (lax.div(owner, plane) * plane + step) * most + rank
        wanted = wanted + jnp.where(lane == owner * most + rank, rows_asked[number], 0)
    wanted_ref[...] = wanted
    own_ids = pltpu.make_async_copy(wanted_ref, wanted_smem, wanted_sem)

    def project_passages(tile, before_keys=None, before_values=None):
        normed = row_norm(store_buf[tile], passage_gain_ref[...].astype(jnp.float32)[None, :])
        if before_keys is not None:
            before_keys()
        key_gain = key_gain_ref[...].astype(jnp.float32)[None, :]
        keys = head_norm(dot32(normed, key_w[...]), key_gain)
        if before_values is not None:
            before_values()
        values = dot32(normed, value_w[...]).astype(jnp.bfloat16)
        rows = pl.ds(tile * tile_passages, tile_passages)
        columns[0][rows, :, :width] = keys.reshape(tile_passages, passage_len, width)
        columns[0][rows, :, width:] = values.reshape(tile_passages, passage_len, width)

    def first_loads():
        loads[1].wait()
        start_loads()

    def start_loads():
        for tile in range(1, tiles):
            store_copy(tile).start()
        x_copy.start()
        for load in loads[2:]:
            load.start()

    store_copy(0).wait()
    project_passages(0, loads[0].wait, first_loads)
    pl.semaphore_wait(barrier, met)

    def far_row(other, home):
        near = jnp.minimum(home, REACH) + REACH + 1
        return jnp.where(other < home, other, jnp.maximum(other - near, 0))

    def for_far(action):
        for other in far_planes:

            @pl.when(is_far(other))
            def _(other=other):
                action(other)

    def ids_copy(st, row, send, recv):
        return pltpu.make_async_remote_copy(
            src_ref=wanted_ref,
            dst_ref=ids_in.at[row],
            send_sem=ids_send.at[send],
            recv_sem=ids_recv.at[recv],
            device_id=(st, tp),
            device_id_type=MESH,
        )

    def ids_rows(other):
        if other is None:
            return pl.ds(1, plane - 1), 0
        row = far_row(other, z)
        return pl.ds(plane * (1 + row), plane), 1 + row

    def ids_all(other=None):
        rows, sem = ids_rows(other)
        return pltpu.make_async_remote_copy(
            src_ref=ids_in.at[rows],
            dst_ref=ids_in.at[rows],
            send_sem=ids_send.at[sem],
            recv_sem=ids_recv.at[sem],
            device_id=(me, 1 - tp),
            device_id_type=MESH,
        )

    def ids_local(other=None):
        rows, sem = ids_rows(other)
        return pltpu.make_async_copy(ids_in.at[rows], ids_smem.at[rows], ids_copy_sem.at[sem])

    def send_ids():
        for step in range(1, plane):
            ids_copy(z * plane + asker_place(step), step, 0, 0).start()

        def send_far_ids(other):
            there = far_row(z, other)
            for step in range(plane):
                ids_copy(
                    other * plane + asker_place(step),
                    plane * (1 + there) + step,
                    1 + far_row(other, z),
                    1 + there,
                ).start()

        for_far(send_far_ids)

    def hop(level, up, tile, count=1):
        source = columns[-level if up else level]
        target = columns[-level - 1 if up else level + 1]
        rows = pl.ds(tile * tile_passages, count * tile_passages)
        return pltpu.make_async_remote_copy(
            src_ref=source.at[rows],
            dst_ref=target.at[rows],
            send_sem=hop_send.at[level, int(up)],
            recv_sem=hop_recv.at[level, int(up), tile],
            device_id=(me + plane if up else me - plane, tp),
            device_id_type=MESH,
        )

    def sends(level, up):
        if up:
            return (z >= level) & (z < depth - 1)
        return (z <= depth - 1 - level) & (z > 0)

    def gets(level, up):
        if up:
            return z >= level + 1
        return z <= depth - 2 - level

    def start_hop(level, tile):
        for up in (True, False):

            @pl.when(sends(level, up))
            def _(up=up):
                hop(level, up, tile).start()

    def await_hop(level, tile):
        for up in (True, False):

            @pl.when(gets(level, up))
            def _(up=up):
                hop(level, up, tile).wait_recv()

    def end_hop(level):
        for up in (True, False):

            @pl.when(sends(level, up))
            def _(up=up):
                hop(level, up, 0, tiles).wait_send()

    own_ids.start()
    send_ids()
    start_hop(0, 0)

    swap = pltpu.make_async_remote_copy(
        src_ref=tokens_hbm,
        dst_ref=x_buf.at[:, mine],
        send_sem=tp_send.at[0],
        recv_sem=tp_recv.at[0],
        device_id=(me, 1 - tp),
        device_id_type=MESH,
    )
    swap.start()

    @pl.loop(1, tiles)
    def _(tile):
        store_copy(tile).wait()
        project_passages(tile)
        start_hop(0, tile)

    def take_ids(other=None):
        ids_all(other).wait_recv()
        ids_local(other).start()

    take_ids()
    for_far(take_ids)
    ids_local().wait()
    for_far(lambda other: ids_local(other).wait())
    own_ids.wait()

    def plane_copy(offset, step):
        return pltpu.make_async_remote_copy(
            src_ref=picked.at[offset + REACH, step - 1],
            dst_ref=slots.at[z + offset, step],
            send_sem=plane_send.at[offset + REACH],
            recv_sem=plane_recv.at[offset + REACH],
            device_id=(z * plane + reader_place(step), tp),
            device_id_type=MESH,
        )

    def plane_all(offset):
        return pltpu.make_async_remote_copy(
            src_ref=picked.at[offset + REACH],
            dst_ref=slots.at[z + offset, pl.ds(1, plane - 1)],
            send_sem=plane_send.at[offset + REACH],
            recv_sem=plane_recv.at[offset + REACH],
            device_id=(me, 1 - tp),
            device_id_type=MESH,
        )

    def held(offset):
        return (z + offset >= 0) & (z + offset < depth)

    def deliver(offset):
        @pl.when(held(offset))
        def _():
            owner = (z + offset) * plane + p
            for step in range(plane - 1, -1, -1):
                for rank in range(most):
                    entry = owner * most + rank
                    if step == 0:
                        index = wanted_smem[0, entry]
                        slots[z + offset, 0, rank] = columns[offset][index]
                    else:
                        index = ids_smem[step, 0, entry]
                        picked[offset + REACH, step - 1, rank] = columns[offset][index]
            for step in range(plane - 1, 0, -1):
                plane_copy(offset, step).start()

    def stage_copy(other, step):
        return pltpu.make_async_remote_copy(
            src_ref=far_picked.at[far_row(other, z), step - 1],
            dst_ref=far_stage.at[far_row(other, z), step],
            send_sem=stage_send.at[far_row(other, z)],
            recv_sem=stage_recv.at[far_row(other, z)],
            device_id=(z * plane + reader_place(step), tp),
            device_id_type=MESH,
        )

    def stage_all(other):
        return pltpu.make_async_remote_copy(
            src_ref=far_picked.at[far_row(other, z)],
            dst_ref=far_stage.at[far_row(other, z), pl.ds(1, plane - 1)],
            send_sem=stage_send.at[far_row(other, z)],
            recv_sem=stage_recv.at[far_row(other, z)],
            device_id=(me, 1 - tp),
            device_id_type=MESH,
        )

    def far_copy(other, source):
        return pltpu.make_async_remote_copy(
            src_ref=far_stage.at[far_row(other, z)],
            dst_ref=slots.at[source],
            send_sem=far_send.at[other],
            recv_sem=far_recv.at[source],
            device_id=(other * plane + p, tp),
            device_id_type=MESH,
        )

    def stage_far(other):
        for step in range(plane - 1, -1, -1):
            row = plane * (1 + far_row(other, z)) + step
            for rank in range(most):
                block = columns[0][ids_smem[row, 0, me * most + rank]]
                if step == 0:
                    far_stage[far_row(other, z), 0, rank] = block
                else:
                    far_picked[far_row(other, z), step - 1, rank] = block
        for step in range(plane - 1, 0, -1):
            stage_copy(other, step).start()

    def send_far(other):
        stage_all(other).wait_recv()
        far_copy(other, z).start()

    deliver(0)
    for_far(stage_far)

    for load in loads[2:5]:
        load.wait()
    x_copy.wait()
    swap.wait()
    taps = taps_ref.shape[0]
    lead = -(-(taps - 1) // 8) * 8
    length = tokens // SEQS_DEV
    channels = padded.shape[2]
    token_tile = min(256, length)
    per_sequence = length // token_tile
    for sequence in range(SEQS_DEV):
        padded[sequence, :lead, :] = jnp.zeros((lead, channels), jnp.float32)
        padded[sequence, lead + length :, :] = jnp.zeros((8, channels), jnp.float32)

    def project(tile):
        rows = pl.ds(pl.multiple_of(tile * token_tile, token_tile), token_tile)
        normed = row_norm(x_buf[rows, :], norm_gain_ref[...].astype(jnp.float32)[None, :])
        queries[rows, :] = head_norm(dot32(normed, query_w[...]), query_gain_ref[...].astype(jnp.float32)[None, :])
        value = dot32(normed, conv_value[...])
        gate = dot32(normed, conv_gate[...])
        gated = (value * jax.nn.sigmoid(gate)).astype(jnp.bfloat16).astype(jnp.float32)
        sequence, part = tile // per_sequence, tile % per_sequence
        start = pl.multiple_of(lead + part * token_tile, 8)
        padded[sequence, pl.ds(start, token_tile), :] = gated

    token_tiles = tokens // token_tile

    @pl.loop(0, token_tiles)
    def _(tile):
        project(tile)

        @pl.when(tile < tiles - 1)
        def _():
            await_hop(0, tile)
            start_hop(1, tile)

    chunk = 64
    span = chunk + lead + 8
    block_width = 256 if channels % 256 == 0 else channels

    def convolve(sequence):
        @pl.loop(0, length // chunk)
        def _(index):
            base = pl.multiple_of(index * chunk, chunk)
            for left in range(0, channels, block_width):
                cols = slice(left, left + block_width)
                window = padded[sequence, pl.ds(base, span), cols]
                total = jnp.zeros((chunk, block_width), jnp.float32)
                for shift in range(8):
                    moved = window if shift == 0 else pltpu.roll(window, span - shift, 0)
                    for start in range(0, lead + 1, 8):
                        tap = start + shift - (lead - taps + 1)
                        if 0 <= tap < taps:
                            weight = taps_ref[tap : tap + 1, cols].astype(jnp.float32)
                            total += weight * moved[start : start + chunk, :]
                out_rows = pl.ds(pl.multiple_of(sequence * length + base, chunk), chunk)
                filtered[out_rows, cols] = total

    convolve(0)
    for tile in range(min(token_tiles, tiles - 1), tiles):
        await_hop(0, tile)
        start_hop(1, tile)
    for distance in range(1, 2):
        deliver(-distance)
        deliver(distance)
    for sequence in range(1, SEQS_DEV):
        convolve(sequence)

    row_tile = 128

    @pl.loop(0, tokens // row_tile)
    def _(tile):
        rows = pl.ds(pl.multiple_of(tile * row_tile, row_tile), row_tile)
        block = filtered[rows, :]
        lane = lax.broadcasted_iota(jnp.int32, (row_tile, 128), 1)
        first = jnp.sum(block, axis=-1, keepdims=True)
        second = jnp.sum(block * block, axis=-1, keepdims=True)
        stats[rows, :] = jnp.where(lane == 0, first, second)

    def tp_copy(number, source, target):
        return pltpu.make_async_remote_copy(
            src_ref=source,
            dst_ref=target,
            send_sem=tp_send.at[number],
            recv_sem=tp_recv.at[number],
            device_id=(me, 1 - tp),
            device_id_type=MESH,
        )

    stats_copy = tp_copy(1, stats, stats_in)
    stats_copy.start()
    loads[5].wait()
    loads[6].wait()
    stats_copy.wait()

    @pl.loop(0, tokens // row_tile)
    def _(tile):
        rows = pl.ds(pl.multiple_of(tile * row_tile, row_tile), row_tile)
        sums = stats[rows, :] + stats_in[rows, :]
        mean = sums[:, 0:1] / C_A
        variance = sums[:, 1:2] / C_A - mean * mean
        scaled = (
            (filtered[rows, :] - mean)
            * lax.rsqrt(variance + LAYER_EPS)
            * ln_gain_ref[...].astype(jnp.float32)[None, :]
        )
        acc[rows, :] = dot32(jax.nn.silu(scaled).astype(jnp.bfloat16), conv_out_w[...])

    for tile in range(tiles):
        await_hop(1, tile)
    for distance in range(2, REACH + 1):
        deliver(-distance)
        deliver(distance)
    for_far(send_far)
    for offset in OFFSETS:

        @pl.when(held(offset))
        def _(offset=offset):
            plane_all(offset).wait_recv()

    for_far(lambda other: far_copy(other, other).wait_recv())

    blocks = slots_ref.shape[0] // passes
    block = tokens // blocks
    lanes = min(128, width)
    per_tile = lanes // MEM_HD
    read_rows = passes * passage_len
    lane_head = lax.broadcasted_iota(jnp.int32, (read_rows, lanes), 1) // MEM_HD
    of_head = [lane_head == head for head in range(per_tile)]
    ones = [jnp.where(inside, 1.0, 0.0).astype(jnp.bfloat16) for inside in of_head]
    gate = jnp.tanh(gate_ref[...].astype(jnp.float32)[None, :])

    def attend(first, count):
        @pl.loop(0, count, unroll=4 if count % 4 == 0 else 1)
        def _(number):
            index = first + number
            rows = pl.ds(pl.multiple_of(index * block, block), block)
            query = queries[rows, :]
            read = []
            for part in range(passes):
                slot = slots_ref[index * passes + part]
                read.append(slots[slot // (plane * most), slot // most % plane, slot % most])
            for left in range(0, width, lanes):
                keys = jnp.concatenate([part[:, left : left + lanes] for part in read], axis=0)
                values = jnp.concatenate(
                    [part[:, width + left : width + left + lanes] for part in read], axis=0
                )
                zeros = jnp.zeros_like(keys)
                split_keys = jnp.concatenate(
                    [jnp.where(inside, keys, zeros) for inside in of_head], axis=0
                )
                scores = lax.dot_general(
                    query[:, left : left + lanes],
                    split_keys,
                    (((1,), (1,)), ((), ())),
                    preferred_element_type=jnp.float32,
                )
                expanded = []
                for head in range(per_tile):
                    mine = scores[:, head * read_rows : (head + 1) * read_rows]
                    top = jnp.max(mine, axis=-1, keepdims=True)
                    expanded.append(jnp.exp((mine - top) * MEM_HD ** (-0.5)))
                weights = jnp.concatenate(expanded, axis=1).astype(jnp.bfloat16)
                split_values = jnp.concatenate(
                    [
                        jnp.concatenate([jnp.where(inside, values, zeros), one], axis=1)
                        for inside, one in zip(of_head, ones)
                    ],
                    axis=0,
                )
                mixed = dot32(weights, split_values)
                attended = mixed[:, :lanes] / mixed[:, lanes:]
                memory[rows, left : left + lanes] = (
                    attended * gate[:, left : left + lanes]
                ).astype(jnp.bfloat16)

    share = tokens // 2
    pieces = tp_send.shape[0] - 2
    piece, few = share // pieces, blocks // 2 // pieces

    def part_copy(number):
        rows = pl.ds(pl.multiple_of(number * piece, piece), piece)
        return tp_copy(2 + number, x_buf.at[rows], back_ref.at[rows])

    def part_of(core, number):
        attend(core * (blocks // 2) + number * few, few)
        rows = pl.ds(pl.multiple_of(core * share + number * piece, piece), piece)
        return (acc[rows, :] + dot32(memory[rows, :], mem_out_w[...])).astype(jnp.bfloat16)

    @pl.loop(0, pieces)
    def _(number):
        x_buf[pl.ds(pl.multiple_of(number * piece, piece), piece), :] = part_of(1 - tp, number)
        part_copy(number).start()

    @pl.loop(0, pieces)
    def _(number):
        keep_ref[pl.ds(pl.multiple_of(number * piece, piece), piece), :] = part_of(tp, number)

    ids_all().wait_send()
    for_far(lambda other: ids_all(other).wait_send())
    for level in range(REACH):
        end_hop(level)
    for offset in OFFSETS:

        @pl.when(held(offset))
        def _(offset=offset):
            plane_all(offset).wait_send()

    def end_far(other):
        stage_all(other).wait_send()
        far_copy(other, z).wait_send()

    for_far(end_far)
    for number in range(pieces):
        part_copy(number).wait()


def add_kernel(keep_ref, back_ref, out_hbm, result, sems):
    pieces, piece = result.shape[:2]
    copies = []
    for number in range(pieces):
        rows = pl.ds(number * piece, piece)
        result[number] = (
            keep_ref[rows, :].astype(jnp.float32) + back_ref[rows, :].astype(jnp.float32)
        ).astype(jnp.bfloat16)
        copies.append(
            pltpu.make_async_copy(result.at[number], out_hbm.at[rows], sems.at[number])
        )
        copies[-1].start()
    for copy in copies:
        copy.wait()


def add_parts(keep, back):
    rows, features = keep.shape
    pieces = 4
    vmem = pl.BlockSpec(memory_space=pltpu.VMEM)
    return pl.pallas_call(
        add_kernel,
        in_specs=[vmem, vmem],
        out_specs=pl.BlockSpec(memory_space=pl.ANY),
        out_shape=jax.ShapeDtypeStruct(keep.shape, jnp.bfloat16),
        scratch_shapes=[
            pltpu.VMEM((pieces, rows // pieces, features), jnp.bfloat16),
            pltpu.SemaphoreType.DMA((pieces,)),
        ],
        compiler_params=pltpu.CompilerParams(vmem_limit_bytes=16 << 20),
        name="add_parts",
    )(keep, back)


def layer(
    tokens,
    passage_ids,
    passage_store,
    norm_gain,
    conv_value_weight,
    conv_gate_weight,
    conv_weight,
    ln_gain,
    query_weight,
    query_gain,
    passage_gain,
    key_weight,
    value_weight,
    key_gain,
    memory_gate,
    conv_out_weight,
    memory_out_weight,
):
    owner_count = lax.axis_size("st")
    depth, plane = split_axis(owner_count)
    store_size, passage_len, features = passage_store.shape
    count, _ = tokens.shape
    width = key_weight.shape[1]
    channels = conv_weight.shape[1]

    request_count = passage_ids.shape[0] * passage_ids.shape[1]
    most = max(1, 2 * request_count // owner_count)
    wide = -(-owner_count * most // 128) * 128

    tile_passages = max(1, min(256 // passage_len, store_size))
    tiles = store_size // tile_passages
    lead = -(-(conv_weight.shape[0] - 1) // 8) * 8
    length = count // SEQS_DEV
    share = count // 2
    pieces = 2
    row = (passage_len, 2 * width)
    bf16, f32 = jnp.bfloat16, jnp.float32
    vmem = pl.BlockSpec(memory_space=pltpu.VMEM)
    smem = pl.BlockSpec(memory_space=pltpu.SMEM)
    anywhere = pl.BlockSpec(memory_space=pl.ANY)
    dma = pltpu.SemaphoreType.DMA
    weights = (
        key_weight,
        value_weight,
        query_weight,
        conv_value_weight,
        conv_gate_weight,
        conv_out_weight,
        memory_out_weight,
    )
    reach = len(OFFSETS)
    far_rows = max(depth - 1 - REACH, 1)
    scratch = (
        [pltpu.VMEM(w.shape, bf16) for w in weights]
        + [
            pltpu.VMEM((tiles, tile_passages * passage_len, features), bf16),
            pltpu.VMEM((count, features), bf16),
            pltpu.VMEM((SEQS_DEV, lead + length + 8, channels), f32),
            pltpu.VMEM((count, channels), f32),
            pltpu.VMEM((count, features), f32),
            pltpu.VMEM((count, width), bf16),
            pltpu.VMEM((count, width), bf16),
            pltpu.VMEM((count, 128), f32),
            pltpu.VMEM((count, 128), f32),
            pltpu.VMEM((1, wide), jnp.int32),
            pltpu.SMEM((1, wide), jnp.int32),
            pltpu.SMEM((request_count,), jnp.int32),
            pltpu.VMEM(((1 + far_rows) * plane, 1, wide), jnp.int32),
            pltpu.SMEM(((1 + far_rows) * plane, 1, wide), jnp.int32),
            pltpu.VMEM((depth, plane, most) + row, bf16),
        ]
        + [pltpu.VMEM((store_size,) + row, bf16) for _ in OFFSETS]
        + [
            pltpu.VMEM((reach, max(plane - 1, 1), most) + row, bf16),
            pltpu.VMEM((far_rows, max(plane - 1, 1), most) + row, bf16),
            pltpu.VMEM((far_rows, plane, most) + row, bf16),
            dma((len(weights),)),
            dma((tiles,)),
            dma,
            dma,
            dma((1 + far_rows,)),
            dma((1 + far_rows,)),
            dma((1 + far_rows,)),
            dma((REACH, 2)),
            dma((REACH, 2, tiles)),
            dma((reach,)),
            dma((reach,)),
            dma((far_rows,)),
            dma((far_rows,)),
            dma((depth,)),
            dma((depth,)),
            dma((2 + pieces,)),
            dma((2 + pieces,)),
        ]
    )
    keep, back = pl.pallas_call(
        functools.partial(layer_kernel, depth, plane, most, passage_ids.shape[1]),
        in_specs=[smem] + [vmem] * 7 + [anywhere] * (2 + len(weights)),
        out_specs=[vmem] * 2,
        out_shape=[pltpu.VMEM((share, features), bf16)] * 2,
        scratch_shapes=scratch,
        compiler_params=pltpu.CompilerParams(
            collective_id=0, has_side_effects=True, vmem_limit_bytes=58 << 20
        ),
        cost_estimate=pl.CostEstimate(
            flops=16 << 30, bytes_accessed=24 << 20, transcendentals=0
        ),
        name="layer",
    )(
        passage_ids.T,
        norm_gain,
        passage_gain,
        key_gain,
        query_gain,
        ln_gain,
        memory_gate,
        conv_weight,
        tokens,
        passage_store.reshape(-1, features),
        *weights,
    )
    return add_parts(keep, back)


def solution(mesh):
    return jax.shard_map(
        layer,
        mesh=mesh,
        in_specs=(
            P("st", "tp"),
            P("st", None),
            P("st", None, None),
            P(),
            P(None, "tp"),
            P(None, "tp"),
            P(None, "tp"),
            P("tp"),
            P(None, "tp"),
            P("tp"),
            P(),
            P(None, "tp"),
            P(None, "tp"),
            P("tp"),
            P("tp"),
            P("tp", None),
            P("tp", None),
        ),
        out_specs=P(("st", "tp"), None),
        check_vma=False,
    )
```

```python
import functools

import jax
import jax.numpy as jnp
from jax import lax
from jax.experimental import pallas as pl
from jax.experimental.pallas import tpu as pltpu
from jax.sharding import PartitionSpec as P

C_A = 1536
MEM_HD = 64
SEQS_DEV = 2
NORM_EPS = 1e-06
LAYER_EPS = 1e-05
REACH = 2
MESH = pl.DeviceIdType.MESH
OFFSETS = tuple(range(-REACH, REACH + 1))


def head_norm(product, gain_row):
    lane = lax.broadcasted_iota(jnp.int32, product.shape, 1)
    squares = product * product
    scale = jnp.zeros_like(product)
    for head in range(product.shape[1] // MEM_HD):
        inside = (lane >= head * MEM_HD) & (lane < (head + 1) * MEM_HD)
        total = jnp.sum(jnp.where(inside, squares, 0.0), axis=-1, keepdims=True)
        scale = jnp.where(inside, lax.rsqrt(total * (1.0 / MEM_HD) + NORM_EPS), scale)
    return (product * scale * gain_row).astype(jnp.bfloat16)


def dot32(left, right):
    return jnp.dot(left, right, preferred_element_type=jnp.float32)


def row_norm(rows, gain_row):
    wide = rows.astype(jnp.float32)
    factor = lax.rsqrt(jnp.mean(wide * wide, axis=-1, keepdims=True) + NORM_EPS)
    return (wide * factor * gain_row).astype(jnp.bfloat16)


def split_axis(count):
    plane = 1
    for size in range(1, count + 1):
        if count % size == 0 and size * size <= count:
            plane = size
    return count // plane, plane


def layer_kernel(
    depth,
    plane,
    most,
    passes,
    ids_ref,
    norm_gain_ref,
    passage_gain_ref,
    key_gain_ref,
    query_gain_ref,
    ln_gain_ref,
    gate_ref,
    taps_ref,
    tokens_hbm,
    store_hbm,
    key_w_hbm,
    value_w_hbm,
    query_w_hbm,
    conv_value_hbm,
    conv_gate_hbm,
    conv_out_hbm,
    mem_out_hbm,
    keep_ref,
    back_ref,
    key_w,
    value_w,
    query_w,
    conv_value,
    conv_gate,
    conv_out_w,
    mem_out_w,
    store_buf,
    x_buf,
    padded,
    filtered,
    acc,
    queries,
    memory,
    stats,
    stats_in,
    wanted_ref,
    wanted_smem,
    slots_ref,
    ids_in,
    ids_smem,
    slots,
    *rest,
):
    columns, rest = dict(zip(OFFSETS, rest[: len(OFFSETS)])), rest[len(OFFSETS) :]
    (
        picked,
        far_picked,
        far_stage,
        load_sem,
        store_sem,
        x_sem,
        wanted_sem,
        ids_copy_sem,
        ids_send,
        ids_recv,
        hop_send,
        hop_recv,
        plane_send,
        plane_recv,
        stage_send,
        stage_recv,
        far_send,
        far_recv,
        tp_send,
        tp_recv,
    ) = rest
    me = lax.axis_index("st")
    tp = lax.axis_index("tp")
    z, p = me // plane, me % plane
    power = plane & (plane - 1) == 0
    passage_len = slots.shape[3]
    store_size = columns[0].shape[0]
    tile_passages = store_buf.shape[1] // passage_len
    tiles = store_size // tile_passages
    tile_rows = tile_passages * passage_len
    tokens, features = x_buf.shape
    half = features // 2
    width = key_w.shape[1]

    def reader_place(step):
        return p ^ step if power else (p + step) % plane

    def asker_place(step):
        return p ^ step if power else (p - step + plane) % plane

    far_planes = [o for o in range(depth) if max(o, depth - 1 - o) > REACH]

    def is_far(other):
        return jnp.abs(other - z) > REACH

    def store_copy(tile):
        return pltpu.make_async_copy(
            store_hbm.at[pl.ds(tile * tile_rows, tile_rows)],
            store_buf.at[tile],
            store_sem.at[tile],
        )

    loads = [
        pltpu.make_async_copy(src, dst, load_sem.at[number])
        for number, (src, dst) in enumerate(
            [
                (key_w_hbm, key_w),
                (value_w_hbm, value_w),
                (query_w_hbm, query_w),
                (conv_value_hbm, conv_value),
                (conv_gate_hbm, conv_gate),
                (conv_out_hbm, conv_out_w),
                (mem_out_hbm, mem_out_w),
            ]
        )
    ]
    mine = pl.ds(pl.multiple_of(tp * half, half), half)
    x_copy = pltpu.make_async_copy(tokens_hbm, x_buf.at[:, mine], x_sem)
    store_copy(0).start()
    loads[0].start()
    loads[1].start()
    barrier = pltpu.get_barrier_semaphore()

    def greet(st, core):
        pl.semaphore_signal(barrier, inc=1, device_id=(st, core), device_id_type=MESH)

    greet(me, 1 - tp)
    for step in range(1, plane):
        greet(z * plane + reader_place(step), tp)

    @pl.when(z > 0)
    def _():
        greet(me - plane, tp)

    @pl.when(z < depth - 1)
    def _():
        greet(me + plane, tp)

    met = 1 + plane - 1 + jnp.where(z > 0, 1, 0) + jnp.where(z < depth - 1, 1, 0)
    for other in far_planes:

        @pl.when(is_far(other))
        def _(other=other):
            for place in range(plane):
                greet(other * plane + place, tp)

        met = met + jnp.where(is_far(other), plane, 0)

    requests = slots_ref.shape[0]
    owners, rows_asked = [], []
    for number in range(requests):
        asked = ids_ref[number % passes, number // passes]
        owners.append(lax.div(asked, store_size))
        rows_asked.append(lax.rem(asked, store_size))
    lane = lax.broadcasted_iota(jnp.int32, wanted_ref.shape, 1)
    wanted = jnp.zeros(wanted_ref.shape, jnp.int32)
    for number, owner in enumerate(owners):
        rank = jnp.int32(0)
        for before in owners[:number]:
            rank = rank + (before == owner).astype(jnp.int32)
        place = lax.rem(owner, plane)
        step = place ^ p if power else lax.rem(p - place + plane, plane)
        slots_ref[number] = (lax.div(owner, plane) * plane + step) * most + rank
        wanted = wanted + jnp.where(lane == owner * most + rank, rows_asked[number], 0)
    wanted_ref[...] = wanted
    own_ids = pltpu.make_async_copy(wanted_ref, wanted_smem, wanted_sem)

    def project_passages(tile, part=0, parts=1):
        taken = tile_rows // parts
        raw = store_buf[tile, part * taken : (part + 1) * taken]
        normed = row_norm(raw, passage_gain_ref[...].astype(jnp.float32)[None, :])
        key_gain = key_gain_ref[...].astype(jnp.float32)[None, :]
        keys = head_norm(dot32(normed, key_w[...]), key_gain)
        values = dot32(normed, value_w[...]).astype(jnp.bfloat16)
        count = tile_passages // parts
        rows = pl.ds(tile * tile_passages + part * count, count)
        columns[0][rows, :, :width] = keys.reshape(count, passage_len, width)
        columns[0][rows, :, width:] = values.reshape(count, passage_len, width)

    loads[0].wait()
    loads[1].wait()
    store_copy(0).wait()
    for tile in range(1, tiles):
        store_copy(tile).start()
    x_copy.start()
    for load in loads[2:]:
        load.start()
    first_parts = 2 if tile_passages % 2 == 0 else 1
    project_passages(0, 0, first_parts)
    pl.semaphore_wait(barrier, met)

    def far_row(other, home):
        near = jnp.minimum(home, REACH) + REACH + 1
        return jnp.where(other < home, other, jnp.maximum(other - near, 0))

    def for_far(action):
        for other in far_planes:

            @pl.when(is_far(other))
            def _(other=other):
                action(other)

    def ids_copy(st, row, send, recv):
        return pltpu.make_async_remote_copy(
            src_ref=wanted_ref,
            dst_ref=ids_in.at[row],
            send_sem=ids_send.at[send],
            recv_sem=ids_recv.at[recv],
            device_id=(st, tp),
            device_id_type=MESH,
        )

    def ids_rows(other):
        if other is None:
            return pl.ds(1, plane - 1), 0
        row = far_row(other, z)
        return pl.ds(plane * (1 + row), plane), 1 + row

    def ids_all(other=None):
        rows, sem = ids_rows(other)
        return pltpu.make_async_remote_copy(
            src_ref=ids_in.at[rows],
            dst_ref=ids_in.at[rows],
            send_sem=ids_send.at[sem],
            recv_sem=ids_recv.at[sem],
            device_id=(me, 1 - tp),
            device_id_type=MESH,
        )

    def ids_local(other=None):
        rows, sem = ids_rows(other)
        return pltpu.make_async_copy(ids_in.at[rows], ids_smem.at[rows], ids_copy_sem.at[sem])

    def send_ids():
        for step in range(1, plane):
            ids_copy(z * plane + asker_place(step), step, 0, 0).start()

        def send_far_ids(other):
            there = far_row(z, other)
            for step in range(plane):
                ids_copy(
                    other * plane + asker_place(step),
                    plane * (1 + there) + step,
                    1 + far_row(other, z),
                    1 + there,
                ).start()

        for_far(send_far_ids)

    def hop(level, up, tile, count=1, part=0, parts=1):
        source = columns[-level if up else level]
        target = columns[-level - 1 if up else level + 1]
        taken = count * tile_passages // parts
        rows = pl.ds(tile * tile_passages + part * taken, taken)
        return pltpu.make_async_remote_copy(
            src_ref=source.at[rows],
            dst_ref=target.at[rows],
            send_sem=hop_send.at[level, int(up)],
            recv_sem=hop_recv.at[level, int(up), tile],
            device_id=(me + plane if up else me - plane, tp),
            device_id_type=MESH,
        )

    def sends(level, up):
        if up:
            return (z >= level) & (z < depth - 1)
        return (z <= depth - 1 - level) & (z > 0)

    def gets(level, up):
        if up:
            return z >= level + 1
        return z <= depth - 2 - level

    def start_hop(level, tile, part=0, parts=1):
        for up in (True, False):

            @pl.when(sends(level, up))
            def _(up=up):
                hop(level, up, tile, 1, part, parts).start()

    def await_hop(level, tile):
        for up in (True, False):

            @pl.when(gets(level, up))
            def _(up=up):
                hop(level, up, tile).wait_recv()

    def end_hop(level):
        for up in (True, False):

            @pl.when(sends(level, up))
            def _(up=up):
                hop(level, up, 0, tiles).wait_send()

    own_ids.start()
    send_ids()
    start_hop(0, 0, 0, first_parts)
    for part in range(1, first_parts):
        project_passages(0, part, first_parts)
        start_hop(0, 0, part, first_parts)

    swap = pltpu.make_async_remote_copy(
        src_ref=tokens_hbm,
        dst_ref=x_buf.at[:, mine],
        send_sem=tp_send.at[0],
        recv_sem=tp_recv.at[0],
        device_id=(me, 1 - tp),
        device_id_type=MESH,
    )
    swap.start()

    @pl.loop(1, tiles)
    def _(tile):
        store_copy(tile).wait()
        project_passages(tile)
        start_hop(0, tile)

    def take_ids(other=None):
        ids_all(other).wait_recv()
        ids_local(other).start()

    take_ids()
    for_far(take_ids)
    ids_local().wait()
    for_far(lambda other: ids_local(other).wait())
    own_ids.wait()

    def plane_copy(offset, step):
        return pltpu.make_async_remote_copy(
            src_ref=picked.at[offset + REACH, step - 1],
            dst_ref=slots.at[z + offset, step],
            send_sem=plane_send.at[offset + REACH],
            recv_sem=plane_recv.at[offset + REACH],
            device_id=(z * plane + reader_place(step), tp),
            device_id_type=MESH,
        )

    def plane_all(offset):
        return pltpu.make_async_remote_copy(
            src_ref=picked.at[offset + REACH],
            dst_ref=slots.at[z + offset, pl.ds(1, plane - 1)],
            send_sem=plane_send.at[offset + REACH],
            recv_sem=plane_recv.at[offset + REACH],
            device_id=(me, 1 - tp),
            device_id_type=MESH,
        )

    def held(offset):
        return (z + offset >= 0) & (z + offset < depth)

    def deliver(offset):
        @pl.when(held(offset))
        def _():
            owner = (z + offset) * plane + p
            for step in range(plane - 1, -1, -1):
                for rank in range(most):
                    entry = owner * most + rank
                    if step == 0:
                        index = wanted_smem[0, entry]
                        slots[z + offset, 0, rank] = columns[offset][index]
                    else:
                        index = ids_smem[step, 0, entry]
                        picked[offset + REACH, step - 1, rank] = columns[offset][index]
            for step in range(plane - 1, 0, -1):
                plane_copy(offset, step).start()

    def stage_copy(other, step):
        return pltpu.make_async_remote_copy(
            src_ref=far_picked.at[far_row(other, z), step - 1],
            dst_ref=far_stage.at[far_row(other, z), step],
            send_sem=stage_send.at[far_row(other, z)],
            recv_sem=stage_recv.at[far_row(other, z)],
            device_id=(z * plane + reader_place(step), tp),
            device_id_type=MESH,
        )

    def stage_all(other):
        return pltpu.make_async_remote_copy(
            src_ref=far_picked.at[far_row(other, z)],
            dst_ref=far_stage.at[far_row(other, z), pl.ds(1, plane - 1)],
            send_sem=stage_send.at[far_row(other, z)],
            recv_sem=stage_recv.at[far_row(other, z)],
            device_id=(me, 1 - tp),
            device_id_type=MESH,
        )

    def far_copy(other, source):
        return pltpu.make_async_remote_copy(
            src_ref=far_stage.at[far_row(other, z)],
            dst_ref=slots.at[source],
            send_sem=far_send.at[other],
            recv_sem=far_recv.at[source],
            device_id=(other * plane + p, tp),
            device_id_type=MESH,
        )

    def stage_far(other):
        for step in range(plane - 1, -1, -1):
            row = plane * (1 + far_row(other, z)) + step
            for rank in range(most):
                block = columns[0][ids_smem[row, 0, me * most + rank]]
                if step == 0:
                    far_stage[far_row(other, z), 0, rank] = block
                else:
                    far_picked[far_row(other, z), step - 1, rank] = block
        for step in range(plane - 1, 0, -1):
            stage_copy(other, step).start()

    def send_far(other):
        stage_all(other).wait_recv()
        far_copy(other, z).start()

    deliver(0)
    for_far(stage_far)

    for load in loads[2:5]:
        load.wait()
    x_copy.wait()
    swap.wait()
    taps = taps_ref.shape[0]
    lead = -(-(taps - 1) // 8) * 8
    length = tokens // SEQS_DEV
    channels = padded.shape[2]
    token_tile = min(256, length)
    per_sequence = length // token_tile
    for sequence in range(SEQS_DEV):
        padded[sequence, :lead, :] = jnp.zeros((lead, channels), jnp.float32)
        padded[sequence, lead + length :, :] = jnp.zeros((8, channels), jnp.float32)

    def project(tile):
        rows = pl.ds(pl.multiple_of(tile * token_tile, token_tile), token_tile)
        normed = row_norm(x_buf[rows, :], norm_gain_ref[...].astype(jnp.float32)[None, :])
        queries[rows, :] = head_norm(dot32(normed, query_w[...]), query_gain_ref[...].astype(jnp.float32)[None, :])
        value = dot32(normed, conv_value[...])
        gate = dot32(normed, conv_gate[...])
        gated = (value * jax.nn.sigmoid(gate)).astype(jnp.bfloat16).astype(jnp.float32)
        sequence, part = tile // per_sequence, tile % per_sequence
        start = pl.multiple_of(lead + part * token_tile, 8)
        padded[sequence, pl.ds(start, token_tile), :] = gated

    token_tiles = tokens // token_tile

    @pl.loop(0, token_tiles)
    def _(tile):
        project(tile)

        @pl.when(tile < tiles - 1)
        def _():
            await_hop(0, tile)
            start_hop(1, tile)

    chunk = 64
    span = chunk + lead + 8
    block_width = 256 if channels % 256 == 0 else channels

    def convolve(sequence):
        @pl.loop(0, length // chunk)
        def _(index):
            base = pl.multiple_of(index * chunk, chunk)
            for left in range(0, channels, block_width):
                cols = slice(left, left + block_width)
                window = padded[sequence, pl.ds(base, span), cols]
                total = jnp.zeros((chunk, block_width), jnp.float32)
                for shift in range(8):
                    moved = window if shift == 0 else pltpu.roll(window, span - shift, 0)
                    for start in range(0, lead + 1, 8):
                        tap = start + shift - (lead - taps + 1)
                        if 0 <= tap < taps:
                            weight = taps_ref[tap : tap + 1, cols].astype(jnp.float32)
                            total += weight * moved[start : start + chunk, :]
                out_rows = pl.ds(pl.multiple_of(sequence * length + base, chunk), chunk)
                filtered[out_rows, cols] = total

    convolve(0)
    for tile in range(min(token_tiles, tiles - 1), tiles):
        await_hop(0, tile)
        start_hop(1, tile)
    for distance in range(1, 2):
        deliver(-distance)
        deliver(distance)
    for sequence in range(1, SEQS_DEV):
        convolve(sequence)

    row_tile = 128

    @pl.loop(0, tokens // row_tile)
    def _(tile):
        rows = pl.ds(pl.multiple_of(tile * row_tile, row_tile), row_tile)
        block = filtered[rows, :]
        lane = lax.broadcasted_iota(jnp.int32, (row_tile, 128), 1)
        first = jnp.sum(block, axis=-1, keepdims=True)
        second = jnp.sum(block * block, axis=-1, keepdims=True)
        stats[rows, :] = jnp.where(lane == 0, first, second)

    def tp_copy(number, source, target):
        return pltpu.make_async_remote_copy(
            src_ref=source,
            dst_ref=target,
            send_sem=tp_send.at[number],
            recv_sem=tp_recv.at[number],
            device_id=(me, 1 - tp),
            device_id_type=MESH,
        )

    stats_copy = tp_copy(1, stats, stats_in)
    stats_copy.start()
    loads[5].wait()
    loads[6].wait()
    stats_copy.wait()

    @pl.loop(0, tokens // row_tile)
    def _(tile):
        rows = pl.ds(pl.multiple_of(tile * row_tile, row_tile), row_tile)
        sums = stats[rows, :] + stats_in[rows, :]
        mean = sums[:, 0:1] / C_A
        variance = sums[:, 1:2] / C_A - mean * mean
        scaled = (
            (filtered[rows, :] - mean)
            * lax.rsqrt(variance + LAYER_EPS)
            * ln_gain_ref[...].astype(jnp.float32)[None, :]
        )
        acc[rows, :] = dot32(jax.nn.silu(scaled).astype(jnp.bfloat16), conv_out_w[...])

    for tile in range(tiles):
        await_hop(1, tile)
    for distance in range(2, REACH + 1):
        deliver(-distance)
        deliver(distance)
    for_far(send_far)
    for offset in OFFSETS:

        @pl.when(held(offset))
        def _(offset=offset):
            plane_all(offset).wait_recv()

    for_far(lambda other: far_copy(other, other).wait_recv())

    blocks = slots_ref.shape[0] // passes
    block = tokens // blocks
    lanes = min(128, width)
    per_tile = lanes // MEM_HD
    read_rows = passes * passage_len
    lane_head = lax.broadcasted_iota(jnp.int32, (read_rows, lanes), 1) // MEM_HD
    of_head = [lane_head == head for head in range(per_tile)]
    ones = [jnp.where(inside, 1.0, 0.0).astype(jnp.bfloat16) for inside in of_head]
    gate = jnp.tanh(gate_ref[...].astype(jnp.float32)[None, :])

    def attend(first, count):
        @pl.loop(0, count, unroll=4 if count % 4 == 0 else 1)
        def _(number):
            index = first + number
            rows = pl.ds(pl.multiple_of(index * block, block), block)
            query = queries[rows, :]
            read = []
            for part in range(passes):
                slot = slots_ref[index * passes + part]
                read.append(slots[slot // (plane * most), slot // most % plane, slot % most])
            for left in range(0, width, lanes):
                keys = jnp.concatenate([part[:, left : left + lanes] for part in read], axis=0)
                values = jnp.concatenate(
                    [part[:, width + left : width + left + lanes] for part in read], axis=0
                )
                zeros = jnp.zeros_like(keys)
                split_keys = jnp.concatenate(
                    [jnp.where(inside, keys, zeros) for inside in of_head], axis=0
                )
                scores = lax.dot_general(
                    query[:, left : left + lanes],
                    split_keys,
                    (((1,), (1,)), ((), ())),
                    preferred_element_type=jnp.float32,
                )
                expanded = []
                for head in range(per_tile):
                    mine = scores[:, head * read_rows : (head + 1) * read_rows]
                    top = jnp.max(mine, axis=-1, keepdims=True)
                    expanded.append(jnp.exp((mine - top) * MEM_HD ** (-0.5)))
                weights = jnp.concatenate(expanded, axis=1).astype(jnp.bfloat16)
                split_values = jnp.concatenate(
                    [
                        jnp.concatenate([jnp.where(inside, values, zeros), one], axis=1)
                        for inside, one in zip(of_head, ones)
                    ],
                    axis=0,
                )
                mixed = dot32(weights, split_values)
                attended = mixed[:, :lanes] / mixed[:, lanes:]
                memory[rows, left : left + lanes] = (
                    attended * gate[:, left : left + lanes]
                ).astype(jnp.bfloat16)

    share = tokens // 2
    pieces = tp_send.shape[0] - 2
    piece, few = share // pieces, blocks // 2 // pieces
    subs = 2
    few_rows = piece // subs

    def part_copy(number):
        rows = pl.ds(pl.multiple_of(number * piece, piece), piece)
        return tp_copy(2 + number, x_buf.at[rows], back_ref.at[rows])

    def part_of(core, number, sub=0, subs=1):
        few_rows = piece // subs
        start = core * share + number * piece + sub * few_rows
        rows = pl.ds(pl.multiple_of(start, few_rows), few_rows)
        return (acc[rows, :] + dot32(memory[rows, :], mem_out_w[...])).astype(jnp.bfloat16)

    @pl.loop(0, pieces)
    def _(number):
        attend((1 - tp) * (blocks // 2) + number * few, few)
        for sub in range(subs):
            rows = pl.ds(pl.multiple_of(number * piece + sub * few_rows, few_rows), few_rows)
            x_buf[rows, :] = part_of(1 - tp, number, sub, subs)
            tp_copy(2 + number, x_buf.at[rows], back_ref.at[rows]).start()

    @pl.loop(0, pieces)
    def _(number):
        attend(tp * (blocks // 2) + number * few, few)
        keep_ref[pl.ds(pl.multiple_of(number * piece, piece), piece), :] = part_of(tp, number)

    ids_all().wait_send()
    for_far(lambda other: ids_all(other).wait_send())
    for level in range(REACH):
        end_hop(level)
    for offset in OFFSETS:

        @pl.when(held(offset))
        def _(offset=offset):
            plane_all(offset).wait_send()

    def end_far(other):
        stage_all(other).wait_send()
        far_copy(other, z).wait_send()

    for_far(end_far)
    for number in range(pieces):
        part_copy(number).wait()


def add_kernel(keep_ref, back_ref, out_hbm, result, sems):
    pieces, piece = result.shape[:2]
    copies = []
    for number in range(pieces):
        rows = pl.ds(number * piece, piece)
        result[number] = (
            keep_ref[rows, :].astype(jnp.float32) + back_ref[rows, :].astype(jnp.float32)
        ).astype(jnp.bfloat16)
        copies.append(
            pltpu.make_async_copy(result.at[number], out_hbm.at[rows], sems.at[number])
        )
        copies[-1].start()
    for copy in copies:
        copy.wait()


def add_parts(keep, back):
    rows, features = keep.shape
    pieces = 4
    vmem = pl.BlockSpec(memory_space=pltpu.VMEM)
    return pl.pallas_call(
        add_kernel,
        in_specs=[vmem, vmem],
        out_specs=pl.BlockSpec(memory_space=pl.ANY),
        out_shape=jax.ShapeDtypeStruct(keep.shape, jnp.bfloat16),
        scratch_shapes=[
            pltpu.VMEM((pieces, rows // pieces, features), jnp.bfloat16),
            pltpu.SemaphoreType.DMA((pieces,)),
        ],
        compiler_params=pltpu.CompilerParams(vmem_limit_bytes=16 << 20),
        name="add_parts",
    )(keep, back)


def layer(
    tokens,
    passage_ids,
    passage_store,
    norm_gain,
    conv_value_weight,
    conv_gate_weight,
    conv_weight,
    ln_gain,
    query_weight,
    query_gain,
    passage_gain,
    key_weight,
    value_weight,
    key_gain,
    memory_gate,
    conv_out_weight,
    memory_out_weight,
):
    owner_count = lax.axis_size("st")
    depth, plane = split_axis(owner_count)
    store_size, passage_len, features = passage_store.shape
    count, _ = tokens.shape
    width = key_weight.shape[1]
    channels = conv_weight.shape[1]

    request_count = passage_ids.shape[0] * passage_ids.shape[1]
    most = max(1, 2 * request_count // owner_count)
    wide = -(-owner_count * most // 128) * 128

    tile_passages = max(1, min(256 // passage_len, store_size))
    tiles = store_size // tile_passages
    lead = -(-(conv_weight.shape[0] - 1) // 8) * 8
    length = count // SEQS_DEV
    share = count // 2
    pieces = 2
    row = (passage_len, 2 * width)
    bf16, f32 = jnp.bfloat16, jnp.float32
    vmem = pl.BlockSpec(memory_space=pltpu.VMEM)
    smem = pl.BlockSpec(memory_space=pltpu.SMEM)
    anywhere = pl.BlockSpec(memory_space=pl.ANY)
    dma = pltpu.SemaphoreType.DMA
    weights = (
        key_weight,
        value_weight,
        query_weight,
        conv_value_weight,
        conv_gate_weight,
        conv_out_weight,
        memory_out_weight,
    )
    reach = len(OFFSETS)
    far_rows = max(depth - 1 - REACH, 1)
    scratch = (
        [pltpu.VMEM(w.shape, bf16) for w in weights]
        + [
            pltpu.VMEM((tiles, tile_passages * passage_len, features), bf16),
            pltpu.VMEM((count, features), bf16),
            pltpu.VMEM((SEQS_DEV, lead + length + 8, channels), f32),
            pltpu.VMEM((count, channels), f32),
            pltpu.VMEM((count, features), f32),
            pltpu.VMEM((count, width), bf16),
            pltpu.VMEM((count, width), bf16),
            pltpu.VMEM((count, 128), f32),
            pltpu.VMEM((count, 128), f32),
            pltpu.VMEM((1, wide), jnp.int32),
            pltpu.SMEM((1, wide), jnp.int32),
            pltpu.SMEM((request_count,), jnp.int32),
            pltpu.VMEM(((1 + far_rows) * plane, 1, wide), jnp.int32),
            pltpu.SMEM(((1 + far_rows) * plane, 1, wide), jnp.int32),
            pltpu.VMEM((depth, plane, most) + row, bf16),
        ]
        + [pltpu.VMEM((store_size,) + row, bf16) for _ in OFFSETS]
        + [
            pltpu.VMEM((reach, max(plane - 1, 1), most) + row, bf16),
            pltpu.VMEM((far_rows, max(plane - 1, 1), most) + row, bf16),
            pltpu.VMEM((far_rows, plane, most) + row, bf16),
            dma((len(weights),)),
            dma((tiles,)),
            dma,
            dma,
            dma((1 + far_rows,)),
            dma((1 + far_rows,)),
            dma((1 + far_rows,)),
            dma((REACH, 2)),
            dma((REACH, 2, tiles)),
            dma((reach,)),
            dma((reach,)),
            dma((far_rows,)),
            dma((far_rows,)),
            dma((depth,)),
            dma((depth,)),
            dma((2 + pieces,)),
            dma((2 + pieces,)),
        ]
    )
    keep, back = pl.pallas_call(
        functools.partial(layer_kernel, depth, plane, most, passage_ids.shape[1]),
        in_specs=[smem] + [vmem] * 7 + [anywhere] * (2 + len(weights)),
        out_specs=[vmem] * 2,
        out_shape=[pltpu.VMEM((share, features), bf16)] * 2,
        scratch_shapes=scratch,
        compiler_params=pltpu.CompilerParams(
            collective_id=0, has_side_effects=True, vmem_limit_bytes=58 << 20
        ),
        cost_estimate=pl.CostEstimate(
            flops=16 << 30, bytes_accessed=24 << 20, transcendentals=0
        ),
        name="layer",
    )(
        passage_ids.T,
        norm_gain,
        passage_gain,
        key_gain,
        query_gain,
        ln_gain,
        memory_gate,
        conv_weight,
        tokens,
        passage_store.reshape(-1, features),
        *weights,
    )
    return add_parts(keep, back)


def solution(mesh):
    return jax.shard_map(
        layer,
        mesh=mesh,
        in_specs=(
            P("st", "tp"),
            P("st", None),
            P("st", None, None),
            P(),
            P(None, "tp"),
            P(None, "tp"),
            P(None, "tp"),
            P("tp"),
            P(None, "tp"),
            P("tp"),
            P(),
            P(None, "tp"),
            P(None, "tp"),
            P("tp"),
            P("tp"),
            P("tp", None),
            P("tp", None),
        ),
        out_specs=P(("st", "tp"), None),
        check_vma=False,
    )
```

```python
import functools

import jax
import jax.numpy as jnp
from jax import lax
from jax.experimental import pallas as pl
from jax.experimental.pallas import tpu as pltpu
from jax.sharding import PartitionSpec as P

C_A = 1536
MEM_HD = 64
SEQS_DEV = 2
NORM_EPS = 1e-06
LAYER_EPS = 1e-05
REACH = 2
MESH = pl.DeviceIdType.MESH
OFFSETS = tuple(range(-REACH, REACH + 1))


def head_norm(product, gain_row):
    lane = lax.broadcasted_iota(jnp.int32, product.shape, 1)
    squares = product * product
    scale = jnp.zeros_like(product)
    for head in range(product.shape[1] // MEM_HD):
        inside = (lane >= head * MEM_HD) & (lane < (head + 1) * MEM_HD)
        total = jnp.sum(jnp.where(inside, squares, 0.0), axis=-1, keepdims=True)
        scale = jnp.where(inside, lax.rsqrt(total * (1.0 / MEM_HD) + NORM_EPS), scale)
    return (product * scale * gain_row).astype(jnp.bfloat16)


def dot32(left, right):
    return jnp.dot(left, right, preferred_element_type=jnp.float32)


def row_norm(rows, gain_row):
    wide = rows.astype(jnp.float32)
    factor = lax.rsqrt(jnp.mean(wide * wide, axis=-1, keepdims=True) + NORM_EPS)
    return (wide * factor * gain_row).astype(jnp.bfloat16)


def split_axis(count):
    plane = 1
    for size in range(1, count + 1):
        if count % size == 0 and size * size <= count:
            plane = size
    return count // plane, plane


def layer_kernel(
    depth,
    plane,
    most,
    passes,
    ids_ref,
    norm_gain_ref,
    passage_gain_ref,
    key_gain_ref,
    query_gain_ref,
    ln_gain_ref,
    gate_ref,
    taps_ref,
    tokens_hbm,
    store_hbm,
    key_w_hbm,
    value_w_hbm,
    query_w_hbm,
    conv_value_hbm,
    conv_gate_hbm,
    conv_out_hbm,
    mem_out_hbm,
    keep_ref,
    back_ref,
    key_w,
    value_w,
    query_w,
    conv_value,
    conv_gate,
    conv_out_w,
    mem_out_w,
    store_buf,
    x_buf,
    padded,
    filtered,
    acc,
    queries,
    memory,
    stats,
    stats_in,
    wanted_ref,
    wanted_smem,
    slots_ref,
    ids_in,
    ids_smem,
    slots,
    *rest,
):
    columns, rest = dict(zip(OFFSETS, rest[: len(OFFSETS)])), rest[len(OFFSETS) :]
    (
        picked,
        far_picked,
        far_stage,
        load_sem,
        store_sem,
        x_sem,
        wanted_sem,
        ids_copy_sem,
        ids_send,
        ids_recv,
        hop_send,
        hop_recv,
        plane_send,
        plane_recv,
        stage_send,
        stage_recv,
        far_send,
        far_recv,
        tp_send,
        tp_recv,
    ) = rest
    me = lax.axis_index("st")
    tp = lax.axis_index("tp")
    z, p = me // plane, me % plane
    power = plane & (plane - 1) == 0
    passage_len = slots.shape[3]
    store_size = columns[0].shape[0]
    tile_passages = store_buf.shape[1] // passage_len
    tiles = store_size // tile_passages
    tile_rows = tile_passages * passage_len
    tokens, features = x_buf.shape
    half = features // 2
    width = key_w.shape[1]

    def reader_place(step):
        return p ^ step if power else (p + step) % plane

    def asker_place(step):
        return p ^ step if power else (p - step + plane) % plane

    far_planes = [o for o in range(depth) if max(o, depth - 1 - o) > REACH]

    def is_far(other):
        return jnp.abs(other - z) > REACH

    def store_copy(tile):
        return pltpu.make_async_copy(
            store_hbm.at[pl.ds(tile * tile_rows, tile_rows)],
            store_buf.at[tile],
            store_sem.at[tile],
        )

    loads = [
        pltpu.make_async_copy(src, dst, load_sem.at[number])
        for number, (src, dst) in enumerate(
            [
                (key_w_hbm, key_w),
                (value_w_hbm, value_w),
                (query_w_hbm, query_w),
                (conv_value_hbm, conv_value),
                (conv_gate_hbm, conv_gate),
                (conv_out_hbm, conv_out_w),
                (mem_out_hbm, mem_out_w),
            ]
        )
    ]
    mine = pl.ds(pl.multiple_of(tp * half, half), half)
    x_copy = pltpu.make_async_copy(tokens_hbm, x_buf.at[:, mine], x_sem)
    store_copy(0).start()
    loads[0].start()
    loads[1].start()
    barrier = pltpu.get_barrier_semaphore()

    def greet(st, core):
        pl.semaphore_signal(barrier, inc=1, device_id=(st, core), device_id_type=MESH)

    greet(me, 1 - tp)
    for step in range(1, plane):
        greet(z * plane + reader_place(step), tp)

    @pl.when(z > 0)
    def _():
        greet(me - plane, tp)

    @pl.when(z < depth - 1)
    def _():
        greet(me + plane, tp)

    met = 1 + plane - 1 + jnp.where(z > 0, 1, 0) + jnp.where(z < depth - 1, 1, 0)
    for other in far_planes:

        @pl.when(is_far(other))
        def _(other=other):
            for place in range(plane):
                greet(other * plane + place, tp)

        met = met + jnp.where(is_far(other), plane, 0)

    requests = slots_ref.shape[0]
    owners, rows_asked = [], []
    for number in range(requests):
        asked = ids_ref[number % passes, number // passes]
        owners.append(lax.div(asked, store_size))
        rows_asked.append(lax.rem(asked, store_size))
    lane = lax.broadcasted_iota(jnp.int32, wanted_ref.shape, 1)
    wanted = jnp.zeros(wanted_ref.shape, jnp.int32)
    for number, owner in enumerate(owners):
        rank = jnp.int32(0)
        for before in owners[:number]:
            rank = rank + (before == owner).astype(jnp.int32)
        place = lax.rem(owner, plane)
        step = place ^ p if power else lax.rem(p - place + plane, plane)
        slots_ref[number] = (lax.div(owner, plane) * plane + step) * most + rank
        wanted = wanted + jnp.where(lane == owner * most + rank, rows_asked[number], 0)
    wanted_ref[...] = wanted
    own_ids = pltpu.make_async_copy(wanted_ref, wanted_smem, wanted_sem)

    def project_passages(tile, part=0, parts=1):
        taken = tile_rows // parts
        raw = store_buf[tile, part * taken : (part + 1) * taken]
        normed = row_norm(raw, passage_gain_ref[...].astype(jnp.float32)[None, :])
        key_gain = key_gain_ref[...].astype(jnp.float32)[None, :]
        keys = head_norm(dot32(normed, key_w[...]), key_gain)
        values = dot32(normed, value_w[...]).astype(jnp.bfloat16)
        count = tile_passages // parts
        rows = pl.ds(tile * tile_passages + part * count, count)
        columns[0][rows, :, :width] = keys.reshape(count, passage_len, width)
        columns[0][rows, :, width:] = values.reshape(count, passage_len, width)

    loads[0].wait()
    loads[1].wait()
    store_copy(0).wait()
    for tile in range(1, tiles):
        store_copy(tile).start()
    x_copy.start()
    for load in loads[2:]:
        load.start()
    first_parts = 2 if tile_passages % 2 == 0 else 1
    project_passages(0, 0, first_parts)
    pl.semaphore_wait(barrier, met)

    def far_row(other, home):
        near = jnp.minimum(home, REACH) + REACH + 1
        return jnp.where(other < home, other, jnp.maximum(other - near, 0))

    def for_far(action):
        for other in far_planes:

            @pl.when(is_far(other))
            def _(other=other):
                action(other)

    def ids_copy(st, row, send, recv):
        return pltpu.make_async_remote_copy(
            src_ref=wanted_ref,
            dst_ref=ids_in.at[row],
            send_sem=ids_send.at[send],
            recv_sem=ids_recv.at[recv],
            device_id=(st, tp),
            device_id_type=MESH,
        )

    def ids_rows(other):
        if other is None:
            return pl.ds(1, plane - 1), 0
        row = far_row(other, z)
        return pl.ds(plane * (1 + row), plane), 1 + row

    def ids_all(other=None):
        rows, sem = ids_rows(other)
        return pltpu.make_async_remote_copy(
            src_ref=ids_in.at[rows],
            dst_ref=ids_in.at[rows],
            send_sem=ids_send.at[sem],
            recv_sem=ids_recv.at[sem],
            device_id=(me, 1 - tp),
            device_id_type=MESH,
        )

    def ids_local(other=None):
        rows, sem = ids_rows(other)
        return pltpu.make_async_copy(ids_in.at[rows], ids_smem.at[rows], ids_copy_sem.at[sem])

    def send_ids():
        for step in range(1, plane):
            ids_copy(z * plane + asker_place(step), step, 0, 0).start()

        def send_far_ids(other):
            there = far_row(z, other)
            for step in range(plane):
                ids_copy(
                    other * plane + asker_place(step),
                    plane * (1 + there) + step,
                    1 + far_row(other, z),
                    1 + there,
                ).start()

        for_far(send_far_ids)

    def hop(level, up, tile, count=1, part=0, parts=1):
        source = columns[-level if up else level]
        target = columns[-level - 1 if up else level + 1]
        taken = count * tile_passages // parts
        rows = pl.ds(tile * tile_passages + part * taken, taken)
        return pltpu.make_async_remote_copy(
            src_ref=source.at[rows],
            dst_ref=target.at[rows],
            send_sem=hop_send.at[level, int(up)],
            recv_sem=hop_recv.at[level, int(up), tile],
            device_id=(me + plane if up else me - plane, tp),
            device_id_type=MESH,
        )

    def last_piece(level, up, tail):
        kept = tile_passages - 1
        start = (tiles - 1) * tile_passages + (kept if tail else 0)
        rows = pl.ds(start, 1 if tail else kept)
        return pltpu.make_async_remote_copy(
            src_ref=columns[-level if up else level].at[rows],
            dst_ref=columns[-level - 1 if up else level + 1].at[rows],
            send_sem=hop_send.at[level, int(up)],
            recv_sem=hop_recv.at[level, int(up), tiles if tail else tiles - 1],
            device_id=(me + plane if up else me - plane, tp),
            device_id_type=MESH,
        )

    def for_hops(level, chosen, action):
        for up in (True, False):

            @pl.when(chosen(level, up))
            def _(up=up):
                action(up)

    def start_last(level):
        def both(up):
            last_piece(level, up, False).start()
            last_piece(level, up, True).start()

        for_hops(level, sends, both)

    def sends(level, up):
        if up:
            return (z >= level) & (z < depth - 1)
        return (z <= depth - 1 - level) & (z > 0)

    def gets(level, up):
        if up:
            return z >= level + 1
        return z <= depth - 2 - level

    def start_hop(level, tile, part=0, parts=1):
        for up in (True, False):

            @pl.when(sends(level, up))
            def _(up=up):
                hop(level, up, tile, 1, part, parts).start()

    def await_hop(level, tile):
        for up in (True, False):

            @pl.when(gets(level, up))
            def _(up=up):
                hop(level, up, tile).wait_recv()

    def end_hop(level):
        for up in (True, False):

            @pl.when(sends(level, up))
            def _(up=up):
                hop(level, up, 0, tiles).wait_send()

    own_ids.start()
    send_ids()
    start_hop(0, 0, 0, first_parts)
    for part in range(1, first_parts):
        project_passages(0, part, first_parts)
        start_hop(0, 0, part, first_parts)

    swap = pltpu.make_async_remote_copy(
        src_ref=tokens_hbm,
        dst_ref=x_buf.at[:, mine],
        send_sem=tp_send.at[0],
        recv_sem=tp_recv.at[0],
        device_id=(me, 1 - tp),
        device_id_type=MESH,
    )
    swap.start()

    @pl.loop(1, tiles)
    def _(tile):
        store_copy(tile).wait()
        project_passages(tile)
        start_hop(0, tile)

    def take_ids(other=None):
        ids_all(other).wait_recv()
        ids_local(other).start()

    take_ids()
    for_far(take_ids)
    ids_local().wait()
    for_far(lambda other: ids_local(other).wait())
    own_ids.wait()

    def plane_copy(offset, step):
        return pltpu.make_async_remote_copy(
            src_ref=picked.at[offset + REACH, step - 1],
            dst_ref=slots.at[z + offset, step],
            send_sem=plane_send.at[offset + REACH],
            recv_sem=plane_recv.at[offset + REACH],
            device_id=(z * plane + reader_place(step), tp),
            device_id_type=MESH,
        )

    def plane_all(offset):
        return pltpu.make_async_remote_copy(
            src_ref=picked.at[offset + REACH],
            dst_ref=slots.at[z + offset, pl.ds(1, plane - 1)],
            send_sem=plane_send.at[offset + REACH],
            recv_sem=plane_recv.at[offset + REACH],
            device_id=(me, 1 - tp),
            device_id_type=MESH,
        )

    def held(offset):
        return (z + offset >= 0) & (z + offset < depth)

    def deliver(offset):
        @pl.when(held(offset))
        def _():
            owner = (z + offset) * plane + p
            for step in range(plane - 1, -1, -1):
                for rank in range(most):
                    entry = owner * most + rank
                    if step == 0:
                        index = wanted_smem[0, entry]
                        slots[z + offset, 0, rank] = columns[offset][index]
                    else:
                        index = ids_smem[step, 0, entry]
                        picked[offset + REACH, step - 1, rank] = columns[offset][index]
            for step in range(plane - 1, 0, -1):
                plane_copy(offset, step).start()

    def stage_copy(other, step):
        return pltpu.make_async_remote_copy(
            src_ref=far_picked.at[far_row(other, z), step - 1],
            dst_ref=far_stage.at[far_row(other, z), step],
            send_sem=stage_send.at[far_row(other, z)],
            recv_sem=stage_recv.at[far_row(other, z)],
            device_id=(z * plane + reader_place(step), tp),
            device_id_type=MESH,
        )

    def stage_all(other):
        return pltpu.make_async_remote_copy(
            src_ref=far_picked.at[far_row(other, z)],
            dst_ref=far_stage.at[far_row(other, z), pl.ds(1, plane - 1)],
            send_sem=stage_send.at[far_row(other, z)],
            recv_sem=stage_recv.at[far_row(other, z)],
            device_id=(me, 1 - tp),
            device_id_type=MESH,
        )

    def far_copy(other, source):
        return pltpu.make_async_remote_copy(
            src_ref=far_stage.at[far_row(other, z)],
            dst_ref=slots.at[source],
            send_sem=far_send.at[other],
            recv_sem=far_recv.at[source],
            device_id=(other * plane + p, tp),
            device_id_type=MESH,
        )

    def stage_far(other):
        for step in range(plane - 1, -1, -1):
            row = plane * (1 + far_row(other, z)) + step
            for rank in range(most):
                block = columns[0][ids_smem[row, 0, me * most + rank]]
                if step == 0:
                    far_stage[far_row(other, z), 0, rank] = block
                else:
                    far_picked[far_row(other, z), step - 1, rank] = block
        for step in range(plane - 1, 0, -1):
            stage_copy(other, step).start()

    def send_far(other):
        stage_all(other).wait_recv()
        far_copy(other, z).start()

    deliver(0)
    for_far(stage_far)

    for load in loads[2:5]:
        load.wait()
    x_copy.wait()
    swap.wait()
    taps = taps_ref.shape[0]
    lead = -(-(taps - 1) // 8) * 8
    length = tokens // SEQS_DEV
    channels = padded.shape[2]
    token_tile = min(256, length)
    per_sequence = length // token_tile
    for sequence in range(SEQS_DEV):
        padded[sequence, :lead, :] = jnp.zeros((lead, channels), jnp.float32)
        padded[sequence, lead + length :, :] = jnp.zeros((8, channels), jnp.float32)

    def project(tile):
        rows = pl.ds(pl.multiple_of(tile * token_tile, token_tile), token_tile)
        normed = row_norm(x_buf[rows, :], norm_gain_ref[...].astype(jnp.float32)[None, :])
        queries[rows, :] = head_norm(dot32(normed, query_w[...]), query_gain_ref[...].astype(jnp.float32)[None, :])
        value = dot32(normed, conv_value[...])
        gate = dot32(normed, conv_gate[...])
        gated = (value * jax.nn.sigmoid(gate)).astype(jnp.bfloat16).astype(jnp.float32)
        sequence, part = tile // per_sequence, tile % per_sequence
        start = pl.multiple_of(lead + part * token_tile, 8)
        padded[sequence, pl.ds(start, token_tile), :] = gated

    token_tiles = tokens // token_tile

    @pl.loop(0, token_tiles)
    def _(tile):
        project(tile)

        @pl.when(tile < tiles - 1)
        def _():
            await_hop(0, tile)
            start_hop(1, tile)

    chunk = 64
    span = chunk + lead + 8
    block_width = 256 if channels % 256 == 0 else channels

    def convolve(sequence):
        @pl.loop(0, length // chunk)
        def _(index):
            base = pl.multiple_of(index * chunk, chunk)
            for left in range(0, channels, block_width):
                cols = slice(left, left + block_width)
                window = padded[sequence, pl.ds(base, span), cols]
                total = jnp.zeros((chunk, block_width), jnp.float32)
                for shift in range(8):
                    moved = window if shift == 0 else pltpu.roll(window, span - shift, 0)
                    for start in range(0, lead + 1, 8):
                        tap = start + shift - (lead - taps + 1)
                        if 0 <= tap < taps:
                            weight = taps_ref[tap : tap + 1, cols].astype(jnp.float32)
                            total += weight * moved[start : start + chunk, :]
                out_rows = pl.ds(pl.multiple_of(sequence * length + base, chunk), chunk)
                filtered[out_rows, cols] = total

    convolve(0)
    for tile in range(min(token_tiles, tiles - 1), tiles):
        await_hop(0, tile)
        if tile < tiles - 1:
            start_hop(1, tile)
        else:
            start_last(1)
    for distance in range(1, 2):
        deliver(-distance)
        deliver(distance)
    for sequence in range(1, SEQS_DEV):
        convolve(sequence)

    row_tile = 128

    @pl.loop(0, tokens // row_tile)
    def _(tile):
        rows = pl.ds(pl.multiple_of(tile * row_tile, row_tile), row_tile)
        block = filtered[rows, :]
        lane = lax.broadcasted_iota(jnp.int32, (row_tile, 128), 1)
        first = jnp.sum(block, axis=-1, keepdims=True)
        second = jnp.sum(block * block, axis=-1, keepdims=True)
        stats[rows, :] = jnp.where(lane == 0, first, second)

    def tp_copy(number, source, target):
        return pltpu.make_async_remote_copy(
            src_ref=source,
            dst_ref=target,
            send_sem=tp_send.at[number],
            recv_sem=tp_recv.at[number],
            device_id=(me, 1 - tp),
            device_id_type=MESH,
        )

    stats_copy = tp_copy(1, stats, stats_in)
    stats_copy.start()
    loads[5].wait()
    loads[6].wait()
    stats_copy.wait()

    @pl.loop(0, tokens // row_tile)
    def _(tile):
        rows = pl.ds(pl.multiple_of(tile * row_tile, row_tile), row_tile)
        sums = stats[rows, :] + stats_in[rows, :]
        mean = sums[:, 0:1] / C_A
        variance = sums[:, 1:2] / C_A - mean * mean
        scaled = (
            (filtered[rows, :] - mean)
            * lax.rsqrt(variance + LAYER_EPS)
            * ln_gain_ref[...].astype(jnp.float32)[None, :]
        )
        acc[rows, :] = dot32(jax.nn.silu(scaled).astype(jnp.bfloat16), conv_out_w[...])

    for tile in range(tiles - 1):
        await_hop(1, tile)
    for_hops(1, gets, lambda up: last_piece(1, up, False).wait_recv())
    for_far(send_far)
    for_hops(1, gets, lambda up: last_piece(1, up, True).wait_recv())
    for distance in range(2, REACH + 1):
        deliver(-distance)
        deliver(distance)
    for offset in OFFSETS:

        @pl.when(held(offset))
        def _(offset=offset):
            plane_all(offset).wait_recv()

    for_far(lambda other: far_copy(other, other).wait_recv())

    blocks = slots_ref.shape[0] // passes
    block = tokens // blocks
    lanes = min(128, width)
    per_tile = lanes // MEM_HD
    read_rows = passes * passage_len
    lane_head = lax.broadcasted_iota(jnp.int32, (read_rows, lanes), 1) // MEM_HD
    of_head = [lane_head == head for head in range(per_tile)]
    ones = [jnp.where(inside, 1.0, 0.0).astype(jnp.bfloat16) for inside in of_head]
    gate = jnp.tanh(gate_ref[...].astype(jnp.float32)[None, :])

    def attend(first, count):
        @pl.loop(0, count, unroll=4 if count % 4 == 0 else 1)
        def _(number):
            index = first + number
            rows = pl.ds(pl.multiple_of(index * block, block), block)
            query = queries[rows, :]
            read = []
            for part in range(passes):
                slot = slots_ref[index * passes + part]
                read.append(slots[slot // (plane * most), slot // most % plane, slot % most])
            for left in range(0, width, lanes):
                keys = jnp.concatenate([part[:, left : left + lanes] for part in read], axis=0)
                values = jnp.concatenate(
                    [part[:, width + left : width + left + lanes] for part in read], axis=0
                )
                zeros = jnp.zeros_like(keys)
                split_keys = jnp.concatenate(
                    [jnp.where(inside, keys, zeros) for inside in of_head], axis=0
                )
                scores = lax.dot_general(
                    query[:, left : left + lanes],
                    split_keys,
                    (((1,), (1,)), ((), ())),
                    preferred_element_type=jnp.float32,
                )
                expanded = []
                for head in range(per_tile):
                    mine = scores[:, head * read_rows : (head + 1) * read_rows]
                    top = jnp.max(mine, axis=-1, keepdims=True)
                    expanded.append(jnp.exp((mine - top) * MEM_HD ** (-0.5)))
                weights = jnp.concatenate(expanded, axis=1).astype(jnp.bfloat16)
                split_values = jnp.concatenate(
                    [
                        jnp.concatenate([jnp.where(inside, values, zeros), one], axis=1)
                        for inside, one in zip(of_head, ones)
                    ],
                    axis=0,
                )
                mixed = dot32(weights, split_values)
                attended = mixed[:, :lanes] / mixed[:, lanes:]
                memory[rows, left : left + lanes] = (
                    attended * gate[:, left : left + lanes]
                ).astype(jnp.bfloat16)

    share = tokens // 2
    pieces = tp_send.shape[0] - 2
    piece, few = share // pieces, blocks // 2 // pieces
    subs = 2
    few_rows = piece // subs

    def part_copy(number):
        rows = pl.ds(pl.multiple_of(number * piece, piece), piece)
        return tp_copy(2 + number, x_buf.at[rows], back_ref.at[rows])

    def part_of(core, number, sub=0, subs=1):
        few_rows = piece // subs
        start = core * share + number * piece + sub * few_rows
        rows = pl.ds(pl.multiple_of(start, few_rows), few_rows)
        return (acc[rows, :] + dot32(memory[rows, :], mem_out_w[...])).astype(jnp.bfloat16)

    @pl.loop(0, pieces)
    def _(number):
        attend((1 - tp) * (blocks // 2) + number * few, few)
        for sub in range(subs):
            rows = pl.ds(pl.multiple_of(number * piece + sub * few_rows, few_rows), few_rows)
            x_buf[rows, :] = part_of(1 - tp, number, sub, subs)
            tp_copy(2 + number, x_buf.at[rows], back_ref.at[rows]).start()

    @pl.loop(0, pieces)
    def _(number):
        attend(tp * (blocks // 2) + number * few, few)
        keep_ref[pl.ds(pl.multiple_of(number * piece, piece), piece), :] = part_of(tp, number)

    ids_all().wait_send()
    for_far(lambda other: ids_all(other).wait_send())
    for level in range(REACH):
        end_hop(level)
    for offset in OFFSETS:

        @pl.when(held(offset))
        def _(offset=offset):
            plane_all(offset).wait_send()

    def end_far(other):
        stage_all(other).wait_send()
        far_copy(other, z).wait_send()

    for_far(end_far)
    for number in range(pieces):
        part_copy(number).wait()


def add_kernel(keep_ref, back_ref, out_hbm, result, sems):
    pieces, piece = result.shape[:2]
    copies = []
    for number in range(pieces):
        rows = pl.ds(number * piece, piece)
        result[number] = (
            keep_ref[rows, :].astype(jnp.float32) + back_ref[rows, :].astype(jnp.float32)
        ).astype(jnp.bfloat16)
        copies.append(
            pltpu.make_async_copy(result.at[number], out_hbm.at[rows], sems.at[number])
        )
        copies[-1].start()
    for copy in copies:
        copy.wait()


def add_parts(keep, back):
    rows, features = keep.shape
    pieces = 4
    vmem = pl.BlockSpec(memory_space=pltpu.VMEM)
    return pl.pallas_call(
        add_kernel,
        in_specs=[vmem, vmem],
        out_specs=pl.BlockSpec(memory_space=pl.ANY),
        out_shape=jax.ShapeDtypeStruct(keep.shape, jnp.bfloat16),
        scratch_shapes=[
            pltpu.VMEM((pieces, rows // pieces, features), jnp.bfloat16),
            pltpu.SemaphoreType.DMA((pieces,)),
        ],
        compiler_params=pltpu.CompilerParams(vmem_limit_bytes=16 << 20),
        name="add_parts",
    )(keep, back)


def layer(
    tokens,
    passage_ids,
    passage_store,
    norm_gain,
    conv_value_weight,
    conv_gate_weight,
    conv_weight,
    ln_gain,
    query_weight,
    query_gain,
    passage_gain,
    key_weight,
    value_weight,
    key_gain,
    memory_gate,
    conv_out_weight,
    memory_out_weight,
):
    owner_count = lax.axis_size("st")
    depth, plane = split_axis(owner_count)
    store_size, passage_len, features = passage_store.shape
    count, _ = tokens.shape
    width = key_weight.shape[1]
    channels = conv_weight.shape[1]

    request_count = passage_ids.shape[0] * passage_ids.shape[1]
    most = max(1, 2 * request_count // owner_count)
    wide = -(-owner_count * most // 128) * 128

    tile_passages = max(1, min(256 // passage_len, store_size))
    tiles = store_size // tile_passages
    lead = -(-(conv_weight.shape[0] - 1) // 8) * 8
    length = count // SEQS_DEV
    share = count // 2
    pieces = 2
    row = (passage_len, 2 * width)
    bf16, f32 = jnp.bfloat16, jnp.float32
    vmem = pl.BlockSpec(memory_space=pltpu.VMEM)
    smem = pl.BlockSpec(memory_space=pltpu.SMEM)
    anywhere = pl.BlockSpec(memory_space=pl.ANY)
    dma = pltpu.SemaphoreType.DMA
    weights = (
        key_weight,
        value_weight,
        query_weight,
        conv_value_weight,
        conv_gate_weight,
        conv_out_weight,
        memory_out_weight,
    )
    reach = len(OFFSETS)
    far_rows = max(depth - 1 - REACH, 1)
    scratch = (
        [pltpu.VMEM(w.shape, bf16) for w in weights]
        + [
            pltpu.VMEM((tiles, tile_passages * passage_len, features), bf16),
            pltpu.VMEM((count, features), bf16),
            pltpu.VMEM((SEQS_DEV, lead + length + 8, channels), f32),
            pltpu.VMEM((count, channels), f32),
            pltpu.VMEM((count, features), f32),
            pltpu.VMEM((count, width), bf16),
            pltpu.VMEM((count, width), bf16),
            pltpu.VMEM((count, 128), f32),
            pltpu.VMEM((count, 128), f32),
            pltpu.VMEM((1, wide), jnp.int32),
            pltpu.SMEM((1, wide), jnp.int32),
            pltpu.SMEM((request_count,), jnp.int32),
            pltpu.VMEM(((1 + far_rows) * plane, 1, wide), jnp.int32),
            pltpu.SMEM(((1 + far_rows) * plane, 1, wide), jnp.int32),
            pltpu.VMEM((depth, plane, most) + row, bf16),
        ]
        + [pltpu.VMEM((store_size,) + row, bf16) for _ in OFFSETS]
        + [
            pltpu.VMEM((reach, max(plane - 1, 1), most) + row, bf16),
            pltpu.VMEM((far_rows, max(plane - 1, 1), most) + row, bf16),
            pltpu.VMEM((far_rows, plane, most) + row, bf16),
            dma((len(weights),)),
            dma((tiles,)),
            dma,
            dma,
            dma((1 + far_rows,)),
            dma((1 + far_rows,)),
            dma((1 + far_rows,)),
            dma((REACH, 2)),
            dma((REACH, 2, tiles + 1)),
            dma((reach,)),
            dma((reach,)),
            dma((far_rows,)),
            dma((far_rows,)),
            dma((depth,)),
            dma((depth,)),
            dma((2 + pieces,)),
            dma((2 + pieces,)),
        ]
    )
    keep, back = pl.pallas_call(
        functools.partial(layer_kernel, depth, plane, most, passage_ids.shape[1]),
        in_specs=[smem] + [vmem] * 7 + [anywhere] * (2 + len(weights)),
        out_specs=[vmem] * 2,
        out_shape=[pltpu.VMEM((share, features), bf16)] * 2,
        scratch_shapes=scratch,
        compiler_params=pltpu.CompilerParams(
            collective_id=0, has_side_effects=True, vmem_limit_bytes=58 << 20
        ),
        cost_estimate=pl.CostEstimate(
            flops=16 << 30, bytes_accessed=24 << 20, transcendentals=0
        ),
        name="layer",
    )(
        passage_ids.T,
        norm_gain,
        passage_gain,
        key_gain,
        query_gain,
        ln_gain,
        memory_gate,
        conv_weight,
        tokens,
        passage_store.reshape(-1, features),
        *weights,
    )
    return add_parts(keep, back)


def solution(mesh):
    return jax.shard_map(
        layer,
        mesh=mesh,
        in_specs=(
            P("st", "tp"),
            P("st", None),
            P("st", None, None),
            P(),
            P(None, "tp"),
            P(None, "tp"),
            P(None, "tp"),
            P("tp"),
            P(None, "tp"),
            P("tp"),
            P(),
            P(None, "tp"),
            P(None, "tp"),
            P("tp"),
            P("tp"),
            P("tp", None),
            P("tp", None),
        ),
        out_specs=P(("st", "tp"), None),
        check_vma=False,
    )
```
